256 devices in a mesh: ep: 128 (over z, y, x), tp: 2 (over core).
Axes of the slice: x: 4, y: 4, z: 8, core: 2. Of those that a mesh axis runs over, the one named last changes fastest.
Arguments:
- tokens: bfloat16 [2048, 2048], P('ep'), may hold values from -6 to 6
- cache_keys: bfloat16 [2048, 2, 64, 1024], P('ep', 'tp'), may hold values from -6 to 6
- cache_values: bfloat16 [2048, 2, 64, 1024], P('ep', 'tp'), may hold values from -6 to 6
- cache_lengths: int32 [2048], P('ep'), may hold values from 1 to 1024, as said below
- norm_in: float32 [2048], replicated, may hold values from 0.1 to 1.9
- w_query: bfloat16 [2048, 512], P(None, 'tp'), may hold values from -0.125 to 0.125
- w_key: bfloat16 [2048, 128], P(None, 'tp'), may hold values from -0.125 to 0.125
- w_value: bfloat16 [2048, 128], P(None, 'tp'), may hold values from -0.125 to 0.125
- stick_bias: float32 [8], P('tp'), may hold values from -8 to -1.5
- w_output: bfloat16 [512, 2048], P('tp'), may hold values from -0.75 to 0.75
- norm_mid: float32 [2048], replicated, may hold values from 0.1 to 1.9
- routes: int32 [2048, 6], P('ep'), may hold values from 0 to 127, all different within a row; in each aligned block of 16 rows (0 to 15, 16 to 31, ...) at most 2 rows name the same one
- route_weights: float32 [2048, 6], P('ep'), may hold values from 0.1 to 1
- expert_gate: bfloat16 [128, 2048, 512], P('ep', None, 'tp'), may hold values from -0.125 to 0.125
- expert_up: bfloat16 [128, 2048, 512], P('ep', None, 'tp'), may hold values from -0.125 to 0.125
- expert_down: bfloat16 [128, 512, 2048], P('ep', 'tp'), may hold values from -0.25 to 0.25
- dense_gate: bfloat16 [2048, 256], P('ep'), may hold values from -0.125 to 0.125
- dense_up: bfloat16 [2048, 256], P('ep'), may hold values from -0.125 to 0.125
- dense_down: bfloat16 [256, 2048], P(None, 'ep'), may hold values from -0.375 to 0.375
- mix_gate: float32 [2048], replicated, may hold values from -0.125 to 0.125
- norm_out: float32 [2048], replicated, may hold values from 0.1 to 1.9
Outputs:
- mixed: bfloat16 [2048, 2048], P('ep')
- fresh_keys: bfloat16 [2048, 128], P('ep', 'tp')
- fresh_values: bfloat16 [2048, 128], P('ep', 'tp')
The draws below stay inside these ranges and needn't reach their ends.
Inputs may be any that keep to these rules, and one draw needn't show every extreme that they name: `cache_lengths`: positions at or past a sequence's length are not read. Among the sequences of one index of ep some sequence has length 1024. `routes`: each row names 6 different experts; among the rows of one index of ep (aligned blocks of 16 rows) no expert is named by more than 2 rows, and that bound is reached.
All inputs are finite; a program needn't handle non-finite values.
Results may differ from the reference program's by a relative error of at most 0.015.
Values may be sent and summed in bfloat16 or wider, within the bound.
A program may use at most 64 MiB of HBM per device.

```python
import math
import jax
import jax.numpy as jnp
import numpy as np
from jax import lax

D = 2048
HEADS = 8
KVH = 2
HD = 64
EW = 512
SHARED = 256
TOPK = 6
SEQ_DEV = 16
CACHE = 1024
SEQS = 2048
EXPERTS = 128
CAP = 2
N_EP = 128
N_TP = 2


def draw_cache_lengths(key, part):
    first_key, second_key = jax.random.split(jax.random.fold_in(key, 11))
    drawn_lengths = jax.random.randint(first_key, (SEQS,), 1, CACHE + 1)
    chosen = jax.random.randint(second_key, (SEQS // SEQ_DEV,), 0, SEQ_DEV)
    position = jnp.arange(SEQS)
    is_full = position % SEQ_DEV == jnp.repeat(chosen, SEQ_DEV)
    return jnp.where(is_full, CACHE, drawn_lengths).astype(jnp.int32)


def draw_stick_bias(key, part):
    first_key, second_key, third_key = jax.random.split(jax.random.fold_in(key, 23), 3)
    is_fast = jax.random.randint(first_key, (HEADS,), 0, 2) == 1
    fast_bias = jax.random.uniform(second_key, (HEADS,), jnp.float32, -2.5, -1.5)
    slow_bias = jax.random.uniform(third_key, (HEADS,), jnp.float32, -7.5, -6.0)
    return jnp.where(is_fast, fast_bias, slow_bias).astype(jnp.float32)


def shard_levels(rng, shape, cuts, least, largest):
    loudness, own = 1.0, jax.random.fold_in(rng, 6)
    for dim, shards_of in cuts:
        draws = jnp.exp(jax.random.uniform(jax.random.fold_in(own, dim), (shards_of,), jnp.float32, least / len(cuts), largest / len(cuts)))
        loudness = loudness * jnp.repeat(draws, shape[dim] // shards_of).reshape([-1 if axis == dim else 1 for axis in range(len(shape))])
    return loudness


def deal_out(rng, own, number, rows, amount, top, most, slope):
    sequence = jax.random.permutation(rng, amount)
    packed, ordinary = portions_of(amount, rows * top, most, slope, True), portions_of(amount, rows * top, most, slope, False)
    places = jnp.arange(amount)

    def named(sizes, offset_by):
        used = int((sizes > 0).sum())
        fixed = max(1, used // 4)
        shifted = fixed + (places - fixed + offset_by * (used - fixed)) % max(1, amount - fixed)
        return jnp.zeros((amount,), jnp.int32).at[sequence[jnp.where(places < fixed, places, shifted)]].set(jnp.asarray(sizes, jnp.int32))

    sizes = jnp.where(number % 4 == 0, named(packed, number // 4), named(ordinary, number - number // 4 - 1))
    mixed = jax.random.permutation(jax.random.fold_in(own, 3), amount)
    donor, receiver = mixed[0:amount // 2 * 2:2], mixed[1:amount // 2 * 2:2]
    slack = jnp.minimum(sizes[donor] - 1, most - sizes[receiver]) // 2
    slack = jnp.where((donor == sequence[0]) | (receiver == sequence[0]) | (sizes[receiver] == 0), 0, jnp.maximum(slack, 0))
    shifted = jax.random.randint(jax.random.fold_in(own, 4), (amount // 2,), 0, 1 << 20) % (slack + 1)
    sizes = sizes.at[donor].add(-shifted).at[receiver].add(shifted)
    members = jnp.searchsorted(jnp.cumsum(sizes), jnp.arange(rows * top), side="right").astype(jnp.int32)
    table = members.reshape(top, rows).T
    table = table[jax.random.permutation(jax.random.fold_in(own, 1), rows)]
    offset_by = jax.random.randint(jax.random.fold_in(own, 2), (rows, 1), 0, top)
    return jnp.take_along_axis(table, (jnp.arange(top)[None, :] + offset_by) % top, axis=1)


def portions_of(amount, total, most, slope, full):
    loads = [(1 << 20) // math.isqrt(rank ** slope) + 1 for rank in range(1, amount + 1)]
    largest = most if full else min(most, max(-(-total // amount), total * loads[0] // sum(loads)))
    least = 1 if total - largest >= amount - 1 else 0
    given, surplus = [largest] + [least] * (amount - 1), total - largest - least * (amount - 1)
    while surplus > 0:
        free = [i for i in range(1, amount) if given[i] < largest] or [i for i in range(1, amount) if given[i] < most]
        pool, remaining = sum([loads[i] for i in free]), surplus
        for i in free:
            extra = min(most - given[i], max(1, remaining * loads[i] // pool), surplus)
            given[i] = given[i] + extra
            surplus = surplus - extra
    return np.array(given)


def noise(rng, shape, deviation, reach, pieces=(), kind=jnp.bfloat16):
    level = shard_levels(rng, shape, pieces, -0.22, 0.18) if pieces else 1.0
    entries = jax.random.normal(rng, shape, jnp.float32) * deviation * level
    return jnp.minimum(jnp.maximum(entries, -reach), reach).astype(kind)


def setup_inputs(seed: int = 0) -> dict:
    arg_keys = jax.random.split(jax.random.key(seed), 22)
    tokens = noise(arg_keys[0], (SEQS, D), 1.0, 6.0, ((0, 128),))
    cache_keys = noise(arg_keys[1], (SEQS, KVH, HD, CACHE), 1.0, 6.0, ((0, 128), (1, 2)))
    cache_values = noise(arg_keys[2], (SEQS, KVH, HD, CACHE), 1.0, 6.0, ((0, 128), (1, 2)))
    cache_lengths = draw_cache_lengths(jax.random.fold_in(arg_keys[21], 71), 0)
    norm_in = jnp.clip(1.0 + 0.18 * jax.random.normal(arg_keys[4], (D,), jnp.float32), 0.1, 1.9)
    w_query = noise(arg_keys[5], (D, HEADS * HD), D ** -0.5, 0.125, ((1, 2),))
    w_key = noise(arg_keys[6], (D, KVH * HD), D ** -0.5, 0.125, ((1, 2),))
    w_value = noise(arg_keys[7], (D, KVH * HD), D ** -0.5, 0.125, ((1, 2),))
    stick_bias = draw_stick_bias(jax.random.fold_in(arg_keys[21], 71), 0)
    w_output = noise(arg_keys[9], (HEADS * HD, D), HD ** -0.5, 0.75, ((0, 2),))
    norm_mid = jnp.clip(1.0 + 0.18 * jax.random.normal(arg_keys[10], (D,), jnp.float32), 0.1, 1.9)
    routes_keys = jax.random.split(jax.random.fold_in(arg_keys[11], 1), SEQS // SEQ_DEV)
    routes_turns = jax.random.permutation(jax.random.fold_in(arg_keys[11], 3), SEQS // SEQ_DEV)
    routes = jax.vmap(lambda own, number: deal_out(jax.random.fold_in(arg_keys[11], 2), own, number, SEQ_DEV, EXPERTS, TOPK, CAP, 1))(routes_keys, routes_turns).reshape((SEQS, TOPK))
    route_weights = jnp.clip(jnp.exp(math.log(1.0) - 2.3025851 * jax.random.uniform(arg_keys[12], (SEQS, TOPK), jnp.float32) ** shard_levels(arg_keys[12], (SEQS, TOPK), ((0, 128),), -0.2, 0.2)), 0.1, 1.0)
    expert_gate = noise(arg_keys[13], (EXPERTS, D, EW), D ** -0.5, 0.125, ((0, 128), (2, 2)))
    expert_up = noise(arg_keys[14], (EXPERTS, D, EW), D ** -0.5, 0.125, ((0, 128), (2, 2)))
    expert_down = noise(arg_keys[15], (EXPERTS, EW, D), EW ** -0.5, 0.25, ((0, 128), (1, 2)))
    dense_gate = noise(arg_keys[16], (D, SHARED), D ** -0.5, 0.125, ((0, 128),))
    dense_up = noise(arg_keys[17], (D, SHARED), D ** -0.5, 0.125, ((0, 128),))
    dense_down = noise(arg_keys[18], (SHARED, D), SHARED ** -0.5, 0.375, ((1, 128),))
    mix_gate = noise(arg_keys[19], (D,), D ** -0.5, 0.125, (), jnp.float32)
    norm_out = jnp.clip(1.0 + 0.18 * jax.random.normal(arg_keys[20], (D,), jnp.float32), 0.1, 1.9)
    return dict(tokens=tokens, cache_keys=cache_keys, cache_values=cache_values, cache_lengths=cache_lengths, norm_in=norm_in, w_query=w_query, w_key=w_key, w_value=w_value, stick_bias=stick_bias, w_output=w_output, norm_mid=norm_mid, routes=routes, route_weights=route_weights, expert_gate=expert_gate, expert_up=expert_up, expert_down=expert_down, dense_gate=dense_gate, dense_up=dense_up, dense_down=dense_down, mix_gate=mix_gate, norm_out=norm_out)


def layer_norm(values, gain):
    floats = values.astype(jnp.float32)
    center = lax.optimization_barrier(jnp.mean(floats, -1, keepdims=True))
    spread = lax.optimization_barrier(jnp.mean(jnp.square(floats - center), -1, keepdims=True))
    return (floats - center) * lax.rsqrt(spread + 1e-05) * gain

def rounded(values):
    return lax.optimization_barrier(values.astype(jnp.bfloat16)).astype(jnp.float32)

def reference(tokens, cache_keys, cache_values, cache_lengths, norm_in, w_query, w_key, w_value, stick_bias, w_output, norm_mid, routes, route_weights, expert_gate, expert_up, expert_down, dense_gate, dense_up, dense_down, mix_gate, norm_out):
    normed = layer_norm(tokens, norm_in).astype(jnp.bfloat16)
    queries = jnp.dot(normed, w_query, preferred_element_type=jnp.float32).astype(jnp.bfloat16)
    fresh_keys = jnp.dot(normed, w_key, preferred_element_type=jnp.float32).astype(jnp.bfloat16)
    fresh_values = jnp.dot(normed, w_value, preferred_element_type=jnp.float32).astype(jnp.bfloat16)
    groups = HEADS // KVH
    bias_grid = stick_bias.astype(jnp.float32).reshape(KVH, groups)

    def attend(inputs):
        query_block, key_block, value_block, length_block = inputs
        query_grid = query_block.reshape(SEQ_DEV, KVH, groups, HD).astype(jnp.float32)
        scores = jnp.einsum('bkgd,bkdc->bkgc', query_grid, key_block.astype(jnp.float32)) * HD ** (-0.5)
        scores = scores + bias_grid[None, :, :, None]
        visible = (jnp.arange(CACHE)[None, :] < length_block[:, None])[:, None, None, :]
        log_keep = jnp.where(visible, jax.nn.log_sigmoid(-scores), 0.0)
        later_sum = lax.cumsum(log_keep, axis=3, reverse=True) - log_keep
        stick = jnp.where(visible, jnp.exp(jax.nn.log_sigmoid(scores) + later_sum), 0.0).astype(jnp.bfloat16)
        output = jnp.einsum('bkgc,bkdc->bkgd', stick.astype(jnp.float32), value_block.astype(jnp.float32))
        return output.reshape(SEQ_DEV, HEADS * HD).astype(jnp.bfloat16)
    block_count = SEQS // SEQ_DEV
    attended = lax.map(attend, (queries.reshape(block_count, SEQ_DEV, HEADS * HD), cache_keys.reshape(block_count, SEQ_DEV, KVH, HD, CACHE), cache_values.reshape(block_count, SEQ_DEV, KVH, HD, CACHE), cache_lengths.reshape(block_count, SEQ_DEV)))
    attended = attended.reshape(SEQS, HEADS * HD)
    projected = jnp.dot(attended, w_output, preferred_element_type=jnp.float32)
    hidden = layer_norm(normed.astype(jnp.float32) + projected, norm_mid).astype(jnp.bfloat16)
    slots = N_EP * CAP
    part_width = EW // N_TP

    def run_expert(inputs):
        number, gate_w, up_w, down_w = inputs
        is_hit = routes == number
        weight_sum = lax.optimization_barrier(jnp.sum(jnp.where(is_hit, route_weights, 0.0), axis=1))
        is_used = jnp.any(is_hit, axis=1)
        picked = jnp.nonzero(is_used, size=slots, fill_value=0)[0].astype(jnp.int32)
        is_valid = (jnp.arange(slots) < jnp.sum(is_used.astype(jnp.int32))).astype(weight_sum.dtype)
        token_rows = hidden[picked]
        gate_pre = jnp.dot(token_rows, gate_w, preferred_element_type=jnp.float32)
        up_pre = jnp.dot(token_rows, up_w, preferred_element_type=jnp.float32)
        act = (jax.nn.silu(gate_pre) * up_pre).astype(jnp.bfloat16)
        combined = jnp.zeros((slots, D), gate_pre.dtype)
        for index in range(N_TP):
            partial_value = jnp.dot(act[:, index * part_width:(index + 1) * part_width], down_w[index * part_width:(index + 1) * part_width], preferred_element_type=jnp.float32)
            combined = combined + rounded(partial_value)
        expert_out = rounded(combined)
        return (picked, expert_out * (weight_sum[picked] * is_valid)[:, None])
    picked_all, terms = lax.map(run_expert, (jnp.arange(EXPERTS).astype(jnp.int32), expert_gate, expert_up, expert_down))
    routed = jax.ops.segment_sum(terms.reshape(-1, D), picked_all.reshape(-1), num_segments=SEQS)
    dense_pre = jnp.dot(hidden, dense_gate, preferred_element_type=jnp.float32)
    dense_lin = jnp.dot(hidden, dense_up, preferred_element_type=jnp.float32)
    dense_act = (jax.nn.silu(dense_pre) * dense_lin).astype(jnp.bfloat16)
    dense_out = jnp.dot(dense_act, dense_down, preferred_element_type=jnp.float32)
    mix_weight = jax.nn.sigmoid(jnp.dot(hidden.astype(jnp.float32), mix_gate, precision=lax.Precision.HIGHEST))
    combined_rows = hidden.astype(jnp.float32) + routed + mix_weight[:, None] * dense_out
    mixed = layer_norm(combined_rows, norm_out).astype(jnp.bfloat16)
    return (mixed, fresh_keys, fresh_values)
```

```python
import jax
import jax.numpy as jnp
from jax import lax
from jax.experimental import pallas as pl
from jax.experimental.pallas import tpu as pltpu
from jax.sharding import Mesh
from jax.sharding import PartitionSpec as P

EP = ("ep_0", "ep_1", "ep_2")
MESH = pl.DeviceIdType.MESH
BF = jnp.bfloat16
F32 = jnp.float32
NZ, NY, NX = 8, 4, 4
PLANE = NY * NX
ORDER = (0, 1, 7, 2, 6, 3, 5, 4)
SLOT = {d: i for i, d in enumerate(ORDER)}
OFFS = sorted(
    ((dy, dx) for dy in range(NY) for dx in range(NX) if (dy, dx) != (0, 0)),
    key=lambda o: min(o[0], NY - o[0]) + min(o[1], NX - o[1]),
)
BACK = [OFFS.index(((-dy) % NY, (-dx) % NX)) for dy, dx in OFFS]
NP = len(OFFS)


def dot(a, b):
    return jnp.dot(a, b, preferred_element_type=F32)


def dot_nt(a, b):
    return lax.dot_general(a, b, (((1,), (1,)), ((), ())), preferred_element_type=F32)


def dot_tn(a, b):
    return lax.dot_general(a, b, (((0,), (0,)), ((), ())), preferred_element_type=F32)


def rows(shape):
    return lax.broadcasted_iota(jnp.int32, shape, 0)


def cols(shape):
    return lax.broadcasted_iota(jnp.int32, shape, 1)


def ones_where(mask):
    return jnp.where(mask, 1.0, 0.0).astype(BF)


def norm(v, gain):
    center = jnp.mean(v, -1, keepdims=True)
    off = v - center
    spread = jnp.mean(off * off, -1, keepdims=True)
    return off * lax.rsqrt(spread + 1e-05) * gain


def halves(v):
    high = v.astype(BF)
    return high, (v - high.astype(F32)).astype(BF)


def body(
    tokens, norm_in, norm_mid, norm_out, mix_gate, routes, weights, dgate, dup, ddown,
    lens, bias, ck, cv, wq_h, wk_h, wv_h, wo_h, eg_h, eu_h, ed_h,
    out, fk, fv,
    kb, vb, wq, wk, wv, wo, eg, eu, ed,
    hb, pps, ppr, zb, ob, xb, yb, pbs, pbr, eb, rb, fs, fb, acc, fin,
    rts, rtb, dws, dwb, tb, d2s, d2b, das, dab, d4s, d4b, d4p,
    pm, wh, wl,
    lsem, zss, zrs, pss, prs, css, crs, pairs,
):
    z, y, x, c = (lax.axis_index(a) for a in (*EP, "tp"))
    me = y * NX + x
    o = 1 - c
    mate = (z, y, x, o)

    def along(d):
        return (lax.rem(z + d, NZ), y, x, c)

    def across(k):
        dy, dx = OFFS[k]
        return (z, lax.rem(y + dy, NY), lax.rem(x + dx, NX), c)

    def place(k):
        dy, dx = OFFS[k]
        return lax.rem(y + dy, NY) * NX + lax.rem(x + dx, NX)

    sent = []

    def send(src, dst, ss, rs, dev):
        copy = pltpu.make_async_remote_copy(
            src_ref=src, dst_ref=dst, send_sem=ss, recv_sem=rs, device_id=dev, device_id_type=MESH
        )
        copy.start()
        sent.append(copy)

    def got(dst, rs):
        pltpu.make_async_copy(dst, dst, rs).wait()

    def fetch(n, src, dst):
        copy = pltpu.make_async_copy(src, dst, lsem.at[n])
        copy.start()
        return copy

    l_wq = fetch(0, wq_h, wq)
    l_wk = fetch(1, wk_h, wk)
    l_wv = fetch(2, wv_h, wv)
    l_k = [fetch(3 + b, ck.at[b], kb.at[b]) for b in range(4)]
    l_v = [fetch(7 + b, cv.at[b], vb.at[b]) for b in range(4)]
    l_wo = fetch(11, wo_h, wo)
    l_eg = fetch(12, eg_h, eg)
    l_eu = fetch(13, eu_h, eu)
    l_ed = fetch(14, ed_h, ed)

    barrier = pltpu.get_barrier_semaphore()
    for d in range(1, NZ):
        pl.semaphore_signal(barrier, inc=1, device_id=along(d), device_id_type=MESH)
    for k in range(NP):
        pl.semaphore_signal(barrier, inc=1, device_id=across(k), device_id_type=MESH)
    pl.semaphore_signal(barrier, inc=1, device_id=mate, device_id_type=MESH)

    half = pl.ds(pl.multiple_of(c * 128, 128), 128)
    dws[0:16] = dgate[:, half]
    dws[16:32] = dup[:, half]
    dws[32:48] = ddown[:, half]
    rts[...] = jnp.zeros((16, 128), F32)
    for j in range(8):
        rts[0:6, 16 * j : 16 * j + 16] = routes[...].astype(F32)
        rts[8:14, 16 * j : 16 * j + 16] = weights[...]

    normed = norm(tokens[...].astype(F32), norm_in[...]).astype(BF)
    l_wq.wait()
    queries = dot(normed, wq[...]).astype(BF)
    l_wk.wait()
    fk[...] = dot_nt(normed, wk[...]).astype(BF)
    l_wv.wait()
    fv[...] = dot_nt(normed, wv[...]).astype(BF)

    pl.semaphore_wait(barrier, NZ - 1 + NP + 1)
    for k in range(NP):
        send(dws, dwb.at[me], pss.at[0, k], prs.at[0, BACK[k]], across(k))
    for d in ORDER[1:]:
        s = SLOT[NZ - d]
        send(rts, rtb.at[s], zss.at[0, SLOT[d]], zrs.at[0, s], along(d))
    dwb[me] = dws[...]
    rtb[0] = rts[...]

    wide = (64, 256)
    expand = ones_where(rows((64, 16)) // 4 == cols((64, 16)))
    fold = ones_where(lax.rem(rows((256, 256)), 64) == lax.rem(cols((256, 256)), 64))
    head_of = cols(wide) // 64 == lax.rem(rows(wide), 4)
    seq_of = cols(wide) // 64 == lax.rem(rows(wide) // 4, 4)
    picked = jnp.where(head_of, dot(expand, queries), 0.0).astype(BF)
    grid = jnp.where(seq_of, dot(picked, fold), 0.0).astype(BF)
    parts = []
    for b in range(4):
        l_k[b].wait()
        parts.append(dot(grid[16 * b : 16 * b + 16], kb[b]))
    scores = jnp.concatenate(parts, axis=0) * 0.125
    row = rows((64, 128))
    length = jnp.zeros((64, 128), jnp.int32)
    for s in range(16):
        length = jnp.where(row // 4 == s, lens[s], length)
    offset = jnp.zeros((64, 128), F32)
    for g in range(4):
        offset = jnp.where(lax.rem(row, 4) == g, bias[g], offset)
    later = ones_where(rows((128, 128)) >= cols((128, 128)))
    zs, keeps, seen = [], [], []
    for n in range(8):
        zn = scores[:, 128 * n : 128 * n + 128] + offset
        vis = cols((64, 128)) + 128 * n < length
        soft = jnp.maximum(zn, 0.0) + jnp.log1p(jnp.exp(-jnp.abs(zn)))
        zs.append(zn)
        seen.append(vis)
        keeps.append(jnp.where(vis, soft, 0.0))
    high, low = halves(jnp.concatenate(keeps, axis=0))
    within = dot(high, later) + dot(low, later)
    carry = jnp.zeros((64, 1), F32)
    sticks = [None] * 8
    for n in range(7, -1, -1):
        w = within[64 * n : 64 * n + 64]
        sticks[n] = jnp.where(seen[n], jnp.exp(zs[n] - w - carry), 0.0).astype(BF)
        carry = carry + w[:, 0:1]
    stick = jnp.concatenate(sticks, axis=1)
    parts = []
    for b in range(4):
        l_v[b].wait()
        parts.append(dot_nt(stick[16 * b : 16 * b + 16], vb[b]))
    att = jnp.where(seq_of, jnp.concatenate(parts, axis=0), 0.0).astype(BF)
    att = jnp.where(head_of, dot(att, fold), 0.0).astype(BF)
    gather = ones_where(cols((16, 64)) // 4 == rows((16, 64)))
    attended = dot(gather, att).astype(BF)
    l_wo.wait()
    pps[...] = dot(attended, wo[...])
    send(pps, ppr, css.at[0], crs.at[0], mate)

    for s in range(1, NZ):
        got(rtb.at[s], zrs.at[0, s])
    shape = (128, 64)
    expert = (z * PLANE + rows(shape) // 8).astype(F32)
    ahead = ones_where(
        (rows((64, 64)) < cols((64, 64))) & (rows((64, 64)) // 16 == cols((64, 64)) // 16)
    )
    for w in range(2):
        table = jnp.zeros((16, 64), F32)
        for j in range(4):
            table = jnp.where(cols((16, 64)) // 16 == j, rtb[4 * w + j][:, 0:64], table)
        hit = jnp.zeros(shape, F32)
        share = jnp.zeros(shape, F32)
        for k in range(6):
            same = table[k : k + 1] == expert
            hit = jnp.where(same, 1.0, hit)
            share = jnp.where(same, table[8 + k : 9 + k], share)
        rank = dot(hit.astype(BF), ahead)
        here = (
            (hit > 0.5)
            & (rank == lax.rem(rows(shape), 2).astype(F32))
            & (cols(shape) // 16 == lax.rem(rows(shape), 8) // 2)
        )
        pm[w] = ones_where(here)
        high, low = halves(jnp.where(here, share, 0.0))
        wh[w] = high
        wl[w] = low

    got(ppr, crs.at[0])
    hidden = norm(normed.astype(F32) + (pps[...] + ppr[...]), norm_mid[...]).astype(BF)
    hb[...] = hidden
    own_half = pl.ds(pl.multiple_of(c * 1024, 1024), 1024)
    mate_half = pl.ds(pl.multiple_of(o * 1024, 1024), 1024)
    for d in ORDER[1:]:
        s = SLOT[NZ - d]
        send(hb.at[:, own_half], zb.at[s], zss.at[1, SLOT[d]], zrs.at[1, s], along(d))
    zb[0] = hb[:, own_half]
    for d in ORDER[1:]:
        s = SLOT[NZ - d]
        there = pl.ds(pl.multiple_of(lax.rem(z + d, NZ) * 256, 256), 256)
        send(hb.at[:, there], tb.at[s], zss.at[2, SLOT[d]], zrs.at[2, s], along(d))
    tb[0] = hb[:, pl.ds(pl.multiple_of(z * 256, 256), 256)]
    mixing = jax.nn.sigmoid(jnp.sum(hidden.astype(F32) * mix_gate[...], -1, keepdims=True))

    def dispatch(w):
        for s in range(4 * w, 4 * w + 4):
            if s:
                got(zb.at[s], zrs.at[1, s])
        block = zb[4 * w : 4 * w + 4].reshape(64, 1024)
        going = dot(pm[w], block)
        for q in range(PLANE):
            ob[w, q] = going[8 * q : 8 * q + 8].astype(BF)
        for k in range(NP):
            send(
                ob.at[w, place(k)], xb.at[w, me], pss.at[1 + w, k], prs.at[1 + w, BACK[k]], across(k)
            )
        xb[w, me] = ob[w, me]
        send(ob.at[w, me], yb.at[w, me], css.at[1 + w], crs.at[1 + w], mate)

    def forward(w):
        for k in range(NP):
            slot = place(k)
            got(xb.at[w, slot], prs.at[1 + w, k])
            send(xb.at[w, slot], yb.at[w, slot], pairs.at[0, w, k], pairs.at[1, w, k], mate)

    def experts(w):
        got(yb.at[w, me], crs.at[1 + w])
        for k in range(NP):
            got(yb.at[w, place(k)], pairs.at[1, w, k])
        if w == 0:
            l_eg.wait()
            l_eu.wait()
        mine = xb[w].reshape(128, 1024)
        other = yb[w].reshape(128, 1024)
        gate = dot(mine, eg[own_half, :]) + dot(other, eg[mate_half, :])
        up = dot(mine, eu[own_half, :]) + dot(other, eu[mate_half, :])
        act = (jax.nn.silu(gate) * up).astype(BF)
        if w == 0:
            l_ed.wait()
        pbs[w] = dot(act, ed[:, mate_half]).astype(BF)
        send(pbs.at[w], pbr.at[w], css.at[3 + w], crs.at[3 + w], mate)
        return dot(act, ed[:, own_half]).astype(BF)

    def give_back(w, part):
        got(pbr.at[w], crs.at[3 + w])
        total = part.astype(F32) + pbr[w].astype(F32)
        for q in range(PLANE):
            eb[w, q] = total[8 * q : 8 * q + 8].astype(BF)
        for k in range(NP):
            send(
                eb.at[w, place(k)], rb.at[w, me], pss.at[3 + w, k], prs.at[3 + w, BACK[k]], across(k)
            )
        rb[w, me] = eb[w, me]

    def combine(w):
        for k in range(NP):
            got(rb.at[w, place(k)], prs.at[3 + w, k])
        block = rb[w].reshape(128, 1024)
        part = dot_tn(wh[w], block) + dot_tn(wl[w], block)
        for j in range(4):
            s = 4 * w + j
            piece = part[16 * j : 16 * j + 16]
            if s == 0:
                acc[...] = piece
            else:
                d = ORDER[s]
                t = SLOT[NZ - d]
                fs[s] = piece.astype(BF)
                send(fs.at[s], fb.at[t], zss.at[6, s], zrs.at[6, t], along(d))

    dispatch(0)

    for k in range(NP):
        got(dwb.at[place(k)], prs.at[0, k])
    for s in range(1, NZ):
        got(tb.at[s], zrs.at[2, s])
    column = tb[...].reshape(128, 256)
    pre = dot(column, dwb[:, 0:16, :].reshape(256, 128))
    lin = dot(column, dwb[:, 16:32, :].reshape(256, 128))
    for s in range(NZ):
        d2s[s, :, 0:128] = pre[16 * s : 16 * s + 16]
        d2s[s, :, 128:256] = lin[16 * s : 16 * s + 16]
    for d in ORDER[1:]:
        t = SLOT[NZ - d]
        send(d2s.at[SLOT[d]], d2b.at[t], zss.at[3, SLOT[d]], zrs.at[3, t], along(d))
    d2b[0] = d2s[0]

    dispatch(1)
    forward(0)
    part0 = experts(0)

    for s in range(1, NZ):
        got(d2b.at[s], zrs.at[3, s])
    total = jnp.sum(d2b[...], axis=0)
    das[...] = (jax.nn.silu(total[:, 0:128]) * total[:, 128:256]).astype(BF)
    for d in ORDER[1:]:
        t = SLOT[NZ - d]
        send(das, dab.at[t], zss.at[4, SLOT[d]], zrs.at[4, t], along(d))
    dab[0] = das[...]

    give_back(0, part0)
    forward(1)
    part1 = experts(1)

    for s in range(1, NZ):
        got(dab.at[s], zrs.at[4, s])
    cols_out = dot_nt(dab[...].reshape(128, 128), dwb[:, 32:48, :].reshape(256, 128))
    for s in range(NZ):
        d4s[s] = cols_out[16 * s : 16 * s + 16]
    for d in ORDER[1:]:
        send(d4s.at[SLOT[d]], d4b.at[z], zss.at[5, SLOT[d]], zrs.at[5, SLOT[NZ - d]], along(d))
    d4b[z] = d4s[0]

    give_back(1, part1)
    combine(0)

    for d in ORDER[1:]:
        got(d4b.at[lax.rem(z + d, NZ)], zrs.at[5, SLOT[d]])
    send(d4b, d4p, css.at[5], crs.at[5], mate)

    combine(1)
    got(d4p, crs.at[5])
    mixed = hidden.astype(F32) + mixing * jnp.concatenate(
        [d4b[n] + d4p[n] for n in range(NZ)], axis=1
    )
    total = acc[...]
    for s in range(1, NZ):
        got(fb.at[s], zrs.at[6, s])
        total = total + fb[s].astype(F32)
    fin[:, own_half] = total
    send(fin.at[:, own_half], fin.at[:, own_half], css.at[6], crs.at[6], mate)
    got(fin.at[:, mate_half], crs.at[6])
    out[...] = norm(mixed + fin[...], norm_out[...]).astype(BF)

    for copy in sent:
        copy.wait_send()


def shards(
    tokens, cache_keys, cache_values, cache_lengths, norm_in, w_query, w_key, w_value,
    stick_bias, w_output, norm_mid, routes, route_weights, expert_gate, expert_up,
    expert_down, dense_gate, dense_up, dense_down, mix_gate, norm_out,
):
    vmem = pl.BlockSpec(memory_space=pltpu.VMEM)
    smem = pl.BlockSpec(memory_space=pltpu.SMEM)
    hbm = pl.BlockSpec(memory_space=pl.ANY)
    dma = pltpu.SemaphoreType.DMA
    V = pltpu.VMEM
    return pl.pallas_call(
        body,
        out_shape=(
            jax.ShapeDtypeStruct((16, 2048), BF),
            jax.ShapeDtypeStruct((16, 64), BF),
            jax.ShapeDtypeStruct((16, 64), BF),
        ),
        in_specs=[vmem] * 10 + [smem] * 2 + [hbm] * 9,
        out_specs=(vmem, vmem, vmem),
        scratch_shapes=[
            V((4, 256, 1024), BF),
            V((4, 256, 1024), BF),
            V((2048, 256), BF),
            V((64, 2048), BF),
            V((64, 2048), BF),
            V((256, 2048), BF),
            V((2048, 256), BF),
            V((2048, 256), BF),
            V((256, 2048), BF),
            V((16, 2048), BF),
            V((16, 2048), F32),
            V((16, 2048), F32),
            V((8, 16, 1024), BF),
            V((2, 16, 8, 1024), BF),
            V((2, 16, 8, 1024), BF),
            V((2, 16, 8, 1024), BF),
            V((2, 128, 1024), BF),
            V((2, 128, 1024), BF),
            V((2, 16, 8, 1024), BF),
            V((2, 16, 8, 1024), BF),
            V((8, 16, 1024), BF),
            V((8, 16, 1024), BF),
            V((16, 1024), F32),
            V((16, 2048), F32),
            V((16, 128), F32),
            V((8, 16, 128), F32),
            V((48, 128), BF),
            V((16, 48, 128), BF),
            V((8, 16, 256), BF),
            V((8, 16, 256), F32),
            V((8, 16, 256), F32),
            V((16, 128), BF),
            V((8, 16, 128), BF),
            V((8, 16, 256), F32),
            V((8, 16, 256), F32),
            V((8, 16, 256), F32),
            V((2, 128, 64), BF),
            V((2, 128, 64), BF),
            V((2, 128, 64), BF),
            dma((15,)),
            dma((7, 8)),
            dma((7, 8)),
            dma((5, 15)),
            dma((5, 15)),
            dma((7,)),
            dma((7,)),
            dma((2, 2, 15)),
        ],
        compiler_params=pltpu.CompilerParams(
            collective_id=0, has_side_effects=True, vmem_limit_bytes=67043328
        ),
    )(
        tokens,
        norm_in.reshape(1, -1),
        norm_mid.reshape(1, -1),
        norm_out.reshape(1, -1),
        mix_gate.reshape(1, -1),
        routes.T,
        route_weights.T,
        dense_gate,
        dense_up,
        dense_down.T,
        cache_lengths,
        stick_bias,
        cache_keys.reshape(4, 256, 1024),
        cache_values.reshape(4, 256, 1024),
        w_query,
        w_key.T,
        w_value.T,
        w_output,
        expert_gate.reshape(2048, 256),
        expert_up.reshape(2048, 256),
        expert_down.reshape(256, 2048),
    )


def solution(mesh):
    split = Mesh(
        mesh.devices.reshape(NZ, NY, NX, mesh.shape["tp"]), ("ep_0", "ep_1", "ep_2", "tp")
    )
    return jax.shard_map(
        shards,
        mesh=split,
        in_specs=(
            P(EP, None),
            P(EP, "tp", None, None),
            P(EP, "tp", None, None),
            P(EP),
            P(),
            P(None, "tp"),
            P(None, "tp"),
            P(None, "tp"),
            P("tp"),
            P("tp", None),
            P(),
            P(EP, None),
            P(EP, None),
            P(EP, None, "tp"),
            P(EP, None, "tp"),
            P(EP, "tp", None),
            P(EP, None),
            P(EP, None),
            P(None, EP),
            P(),
            P(),
        ),
        out_specs=(P(EP, None), P(EP, "tp"), P(EP, "tp")),
        check_vma=False,
    )
```

```python
import jax
import jax.numpy as jnp
from jax import lax
from jax.experimental import pallas as pl
from jax.experimental.pallas import tpu as pltpu
from jax.sharding import Mesh
from jax.sharding import PartitionSpec as P

EP = ("ep_0", "ep_1", "ep_2")
MESH = pl.DeviceIdType.MESH
BF = jnp.bfloat16
F32 = jnp.float32
NZ, NY, NX = 8, 4, 4
PLANE = NY * NX
ORDER = (0, 4, 1, 7, 2, 6, 3, 5)
SLOT = {d: i for i, d in enumerate(ORDER)}
OFFS = sorted(
    ((dy, dx) for dy in range(NY) for dx in range(NX) if (dy, dx) != (0, 0)),
    key=lambda o: min(o[0], NY - o[0]) + min(o[1], NX - o[1]),
)
BACK = [OFFS.index(((-dy) % NY, (-dx) % NX)) for dy, dx in OFFS]
NP = len(OFFS)


def dot(a, b):
    return jnp.dot(a, b, preferred_element_type=F32)


def dot_nt(a, b):
    return lax.dot_general(a, b, (((1,), (1,)), ((), ())), preferred_element_type=F32)


def rows(shape):
    return lax.broadcasted_iota(jnp.int32, shape, 0)


def cols(shape):
    return lax.broadcasted_iota(jnp.int32, shape, 1)


def ones_where(mask):
    return jnp.where(mask, 1.0, 0.0).astype(BF)


def norm(v, gain):
    center = jnp.mean(v, -1, keepdims=True)
    off = v - center
    spread = jnp.mean(off * off, -1, keepdims=True)
    return off * lax.rsqrt(spread + 1e-05) * gain


def halves(v):
    high = v.astype(BF)
    return high, (v - high.astype(F32)).astype(BF)


def body(
    tokens_h, norm_in_h, wq_h, wk_h, wv_h, lens_h, bias_h, ck, cv, dgate_h, dup_h, ddown_h,
    routes_h, weights_h, wo_h, norm_mid_h, mix_gate_h, eg_h, eu_h, ed_h, norm_out_h,
    out, fk, fv,
    tokens, norm_in, wq, wk, wv, lens, bias, kb, vb, dgate, dup, ddown,
    routes, weights, wo, norm_mid, mix_gate, eg, eu, ed, norm_out,
    hb, pps, ppr, zb, ob, xb, yb, pbs, pbr, eb, rb, fs, fb, acc, fin,
    rts, rtb, dws, dwb, tb, d2s, d2b, das, dab, d4s, d4b, d4p,
    pm, wh, wl,
    lsem, bank,
):
    z, y, x, c = (lax.axis_index(a) for a in (*EP, "tp"))
    me = y * NX + x
    o = 1 - c
    mate = (z, y, x, o)

    def along(d):
        return (lax.rem(z + d, NZ), y, x, c)

    def across(k):
        dy, dx = OFFS[k]
        return (z, lax.rem(y + dy, NY), lax.rem(x + dx, NX), c)

    def place(k):
        dy, dx = OFFS[k]
        return lax.rem(y + dy, NY) * NX + lax.rem(x + dx, NX)

    flags = {}

    def flag(*name):
        return bank.at[flags.setdefault(name, len(flags))]

    def send(src, dst, out_flag, in_flag, dev):
        pltpu.make_async_remote_copy(
            src_ref=src, dst_ref=dst, send_sem=out_flag, recv_sem=in_flag,
            device_id=dev, device_id_type=MESH,
        ).start()

    def await_bytes(ref, name):
        pltpu.make_async_copy(ref, ref, name).wait()

    reads = {}

    def fetch(name, src, dst):
        copy = pltpu.make_async_copy(src, dst, lsem.at[len(reads)])
        copy.start()
        reads[name] = copy

    def ready(*names):
        for name in names:
            reads[name].wait()

    fetch("tokens", tokens_h, tokens)
    fetch("norm_in", norm_in_h, norm_in)
    fetch("wq", wq_h, wq)
    fetch("wk", wk_h, wk)
    fetch("wv", wv_h, wv)
    fetch("dgate", dgate_h, dgate)
    fetch("dup", dup_h, dup)
    fetch("ddown", ddown_h, ddown)
    fetch("routes", routes_h, routes)
    fetch("weights", weights_h, weights)
    for b in range(4):
        fetch(("k", b), ck.at[b], kb.at[b])
    fetch("lens", lens_h, lens)
    fetch("bias", bias_h, bias)
    for b in range(4):
        fetch(("v", b), cv.at[b], vb.at[b])
    fetch("wo", wo_h, wo)
    fetch("norm_mid", norm_mid_h, norm_mid)
    fetch("mix_gate", mix_gate_h, mix_gate)
    fetch("eg", eg_h, eg)
    fetch("eu", eu_h, eu)
    fetch("ed", ed_h, ed)
    fetch("norm_out", norm_out_h, norm_out)

    barrier = pltpu.get_barrier_semaphore()
    for d in range(1, NZ):
        pl.semaphore_signal(barrier, inc=1, device_id=along(d), device_id_type=MESH)
    for k in range(NP):
        pl.semaphore_signal(barrier, inc=1, device_id=across(k), device_id_type=MESH)
    pl.semaphore_signal(barrier, inc=1, device_id=mate, device_id_type=MESH)

    ready("tokens", "norm_in")
    normed = norm(tokens[...].astype(F32), norm_in[...]).astype(BF)
    ready("wq")
    queries = dot(normed, wq[...]).astype(BF)
    ready("wk")
    fk[...] = dot_nt(normed, wk[...]).astype(BF)
    ready("wv")
    fv[...] = dot_nt(normed, wv[...]).astype(BF)

    half = pl.ds(pl.multiple_of(c * 128, 128), 128)
    ready("dgate", "dup", "ddown", "routes", "weights")
    dws[0:16] = dgate[:, half]
    dws[16:32] = dup[:, half]
    dws[32:48] = ddown[:, half]
    rts[...] = jnp.zeros((16, 128), F32)
    for j in range(8):
        rts[0:6, 16 * j : 16 * j + 16] = routes[...].astype(F32)
        rts[8:14, 16 * j : 16 * j + 16] = weights[...]

    pl.semaphore_wait(barrier, NZ - 1 + NP + 1)
    for k in range(NP):
        send(dws, dwb.at[me], flag("ws"), flag("wr"), across(k))
    for d in ORDER[1:]:
        send(rts, rtb.at[SLOT[NZ - d]], flag("ts"), flag("tr"), along(d))
    dwb[me] = dws[...]
    rtb[0] = rts[...]

    wide = (64, 256)
    expand = ones_where(rows((64, 16)) // 4 == cols((64, 16)))
    fold = ones_where(lax.rem(rows((256, 256)), 64) == lax.rem(cols((256, 256)), 64))
    head_of = cols(wide) // 64 == lax.rem(rows(wide), 4)
    seq_of = cols(wide) // 64 == lax.rem(rows(wide) // 4, 4)
    picked = jnp.where(head_of, dot(expand, queries), 0.0).astype(BF)
    grid = jnp.where(seq_of, dot(picked, fold), 0.0).astype(BF)
    parts = []
    for b in range(4):
        ready(("k", b))
        parts.append(dot(grid[16 * b : 16 * b + 16], kb[b]))
    scores = jnp.concatenate(parts, axis=0) * 0.125
    ready("lens", "bias")
    row = rows((64, 128))
    length = jnp.zeros((64, 128), jnp.int32)
    for s in range(16):
        length = jnp.where(row // 4 == s, lens[s], length)
    offset = jnp.zeros((64, 128), F32)
    for g in range(4):
        offset = jnp.where(lax.rem(row, 4) == g, bias[g], offset)
    later = ones_where(rows((128, 128)) >= cols((128, 128)))
    zs, keeps, seen = [], [], []
    for n in range(8):
        zn = scores[:, 128 * n : 128 * n + 128] + offset
        vis = cols((64, 128)) + 128 * n < length
        soft = jnp.maximum(zn, 0.0) + jnp.log1p(jnp.exp(-jnp.abs(zn)))
        zs.append(zn)
        seen.append(vis)
        keeps.append(jnp.where(vis, soft, 0.0))
    high, low = halves(jnp.concatenate(keeps, axis=0))
    within = dot(high, later) + dot(low, later)
    carry = jnp.zeros((64, 1), F32)
    sticks = [None] * 8
    for n in range(7, -1, -1):
        w = within[64 * n : 64 * n + 64]
        sticks[n] = jnp.where(seen[n], jnp.exp(zs[n] - w - carry), 0.0).astype(BF)
        carry = carry + w[:, 0:1]
    stick = jnp.concatenate(sticks, axis=1)
    parts = []
    for b in range(4):
        ready(("v", b))
        parts.append(dot_nt(stick[16 * b : 16 * b + 16], vb[b]))
    att = jnp.where(seq_of, jnp.concatenate(parts, axis=0), 0.0).astype(BF)
    att = jnp.where(head_of, dot(att, fold), 0.0).astype(BF)
    gather = ones_where(cols((16, 64)) // 4 == rows((16, 64)))
    attended = dot(gather, att).astype(BF)
    ready("wo")
    pps[...] = dot(attended, wo[...])
    send(pps, ppr, flag("ps"), flag("pr"), mate)

    await_bytes(rtb.at[1:8], flag("tr"))
    shape = (128, 64)
    expert = (z * PLANE + rows(shape) // 8).astype(F32)
    ahead = ones_where(
        (rows((64, 64)) < cols((64, 64))) & (rows((64, 64)) // 16 == cols((64, 64)) // 16)
    )
    for w in range(2):
        table = jnp.zeros((16, 64), F32)
        for j in range(4):
            table = jnp.where(cols((16, 64)) // 16 == j, rtb[4 * w + j][:, 0:64], table)
        hit = jnp.zeros(shape, F32)
        share = jnp.zeros(shape, F32)
        for k in range(6):
            same = table[k : k + 1] == expert
            hit = jnp.where(same, 1.0, hit)
            share = jnp.where(same, table[8 + k : 9 + k], share)
        rank = dot(hit.astype(BF), ahead)
        here = (
            (hit > 0.5)
            & (rank == lax.rem(rows(shape), 2).astype(F32))
            & (cols(shape) // 16 == lax.rem(rows(shape), 8) // 2)
        )
        pm[w] = ones_where(here)
        high, low = halves(jnp.transpose(jnp.where(here, share, 0.0)))
        wh[w] = high
        wl[w] = low
    await_bytes(rtb.at[1:8], flag("ts"))
    await_bytes(dwb.at[0:15], flag("ws"))

    own_half = pl.ds(pl.multiple_of(c * 1024, 1024), 1024)
    mate_half = pl.ds(pl.multiple_of(o * 1024, 1024), 1024)
    ready("norm_mid", "mix_gate")
    await_bytes(ppr, flag("pr"))
    hidden = norm(normed.astype(F32) + (pps[...] + ppr[...]), norm_mid[...]).astype(BF)
    hb[...] = hidden
    for d in (4, 1, 7, 3, 5, 2, 6):
        t = SLOT[NZ - d]
        send(hb.at[:, own_half], zb.at[t], flag("zs"), flag("zr", t // 4), along(d))
    zb[0] = hb[:, own_half]
    mixing = jax.nn.sigmoid(jnp.sum(hidden.astype(F32) * mix_gate[...], -1, keepdims=True))
    await_bytes(pps, flag("ps"))

    def dispatch(w):
        await_bytes(zb.at[1:4] if w == 0 else zb.at[4:8], flag("zr", w))
        block = zb[4 * w : 4 * w + 4].reshape(64, 1024)
        going = dot(pm[w], block)
        for q in range(PLANE):
            ob[w, q] = going[8 * q : 8 * q + 8].astype(BF)
        for k in range(NP):
            send(
                ob.at[w, place(k)], xb.at[w, me], flag("xs", w), flag("xr", w, BACK[k]), across(k)
            )
        send(ob.at[w, me], yb.at[w, me], flag("ys", w), flag("yr", w), mate)
        xb[w, me] = ob[w, me]

    def forward(w):
        for k in range(NP):
            slot = place(k)
            await_bytes(xb.at[w, slot], flag("xr", w, k))
            send(xb.at[w, slot], yb.at[w, slot], flag("ys", w), flag("yr", w), mate)

    def experts(w):
        if w == 0:
            ready("eg", "eu", "ed")
        mine = xb[w].reshape(128, 1024)
        gate = dot(mine, eg[own_half, :])
        up = dot(mine, eu[own_half, :])
        await_bytes(xb.at[w, 0:15], flag("xs", w))
        await_bytes(yb.at[w], flag("yr", w))
        other = yb[w].reshape(128, 1024)
        gate = gate + dot(other, eg[mate_half, :])
        up = up + dot(other, eu[mate_half, :])
        act = (jax.nn.silu(gate) * up).astype(BF)
        pbs[w] = dot(act, ed[:, mate_half]).astype(BF)
        send(pbs.at[w], pbr.at[w], flag("bs", w), flag("br", w), mate)
        part = dot(act, ed[:, own_half]).astype(BF)
        await_bytes(yb.at[w], flag("ys", w))
        return part

    def give_back(w, part):
        await_bytes(pbr.at[w], flag("br", w))
        total = part.astype(F32) + pbr[w].astype(F32)
        for q in range(PLANE):
            eb[w, q] = total[8 * q : 8 * q + 8].astype(BF)
        for k in range(NP):
            send(eb.at[w, place(k)], rb.at[w, me], flag("es", w), flag("er", w), across(k))
        rb[w, me] = eb[w, me]
        await_bytes(pbr.at[w], flag("bs", w))

    def combine(w):
        await_bytes(rb.at[w, 0:15], flag("er", w))
        block = rb[w].reshape(128, 1024)
        part = dot(wh[w], block) + dot(wl[w], block)
        for j in range(4):
            s = 4 * w + j
            piece = part[16 * j : 16 * j + 16]
            if s == 0:
                acc[...] = piece
            else:
                d = ORDER[s]
                fs[s] = piece.astype(BF)
                send(fs.at[s], fb.at[SLOT[NZ - d]], flag("fs", w), flag("fr", w), along(d))
        await_bytes(rb.at[w, 0:15], flag("es", w))

    dispatch(0)
    dispatch(1)

    holder = c == z // 4
    features = pl.ds(pl.multiple_of(lax.rem(z, 4) * 256, 256), 256)

    @pl.when(holder)
    def _():
        send(zb.at[:, :, features], tb, flag("cs"), flag("cr"), mate)
        tb[...] = zb[:, :, features]
        await_bytes(tb, flag("cs"))

    await_bytes(dwb.at[0:15], flag("wr"))

    @pl.when(jnp.logical_not(holder))
    def _():
        await_bytes(tb, flag("cr"))

    column = tb[...].reshape(128, 256)
    pre = dot(column, dwb[:, 0:16, :].reshape(256, 128))
    lin = dot(column, dwb[:, 16:32, :].reshape(256, 128))
    for s in range(NZ):
        d2s[s, :, 0:128] = pre[16 * s : 16 * s + 16]
        d2s[s, :, 128:256] = lin[16 * s : 16 * s + 16]
    for d in ORDER[1:]:
        send(d2s.at[SLOT[d]], d2b.at[SLOT[NZ - d]], flag("d2s"), flag("d2r"), along(d))
    d2b[0] = d2s[0]

    forward(0)
    part0 = experts(0)
    give_back(0, part0)
    await_bytes(zb.at[1:8], flag("zs"))
    forward(1)
    part1 = experts(1)

    await_bytes(d2b.at[1:8], flag("d2r"))
    total = jnp.sum(d2b[...], axis=0)
    das[...] = (jax.nn.silu(total[:, 0:128]) * total[:, 128:256]).astype(BF)
    for d in ORDER[1:]:
        send(das, dab.at[SLOT[NZ - d]], flag("d3s"), flag("d3r"), along(d))
    dab[0] = das[...]

    give_back(1, part1)
    combine(0)

    await_bytes(d2b.at[1:8], flag("d2s"))
    await_bytes(dab.at[1:8], flag("d3r"))
    cols_out = dot_nt(dab[...].reshape(128, 128), dwb[:, 32:48, :].reshape(256, 128))
    for s in range(NZ):
        d4s[s] = cols_out[16 * s : 16 * s + 16]
    for d in ORDER[1:]:
        send(d4s.at[SLOT[d]], d4b.at[z], flag("d4s"), flag("d4r"), along(d))
    d4b[z] = d4s[0]
    await_bytes(dab.at[1:8], flag("d3s"))

    combine(1)
    await_bytes(d4b.at[0:7], flag("d4r"))
    send(d4b, d4p, flag("d5s"), flag("d5r"), mate)
    ready("norm_out")
    await_bytes(fb.at[1:4], flag("fr", 0))
    total = acc[...] + fb[1].astype(F32) + fb[2].astype(F32) + fb[3].astype(F32)
    await_bytes(d4p, flag("d5r"))
    mixed = hidden.astype(F32) + mixing * jnp.concatenate(
        [d4b[n] + d4p[n] for n in range(NZ)], axis=1
    )
    await_bytes(d4b.at[0:7], flag("d4s"))
    await_bytes(d4p, flag("d5s"))
    await_bytes(fb.at[1:4], flag("fs", 0))
    await_bytes(fb.at[4:8], flag("fr", 1))
    for s in range(4, NZ):
        total = total + fb[s].astype(F32)
    fin[:, own_half] = total
    send(fin.at[:, own_half], fin.at[:, own_half], flag("us"), flag("ur"), mate)
    await_bytes(fb.at[4:8], flag("fs", 1))
    await_bytes(fin.at[:, mate_half], flag("ur"))
    out[...] = norm(mixed + fin[...], norm_out[...]).astype(BF)
    await_bytes(fin.at[:, own_half], flag("us"))


def shards(
    tokens, cache_keys, cache_values, cache_lengths, norm_in, w_query, w_key, w_value,
    stick_bias, w_output, norm_mid, routes, route_weights, expert_gate, expert_up,
    expert_down, dense_gate, dense_up, dense_down, mix_gate, norm_out,
):
    vmem = pl.BlockSpec(memory_space=pltpu.VMEM)
    hbm = pl.BlockSpec(memory_space=pltpu.HBM)
    dma = pltpu.SemaphoreType.DMA
    V = pltpu.VMEM
    return pl.pallas_call(
        body,
        out_shape=(V((16, 2048), BF), V((16, 64), BF), V((16, 64), BF)),
        in_specs=[hbm] * 21,
        out_specs=(vmem, vmem, vmem),
        scratch_shapes=[
            V((16, 2048), BF),
            V((1, 2048), F32),
            V((2048, 256), BF),
            V((64, 2048), BF),
            V((64, 2048), BF),
            pltpu.SMEM((16,), jnp.int32),
            pltpu.SMEM((4,), F32),
            V((4, 256, 1024), BF),
            V((4, 256, 1024), BF),
            V((16, 256), BF),
            V((16, 256), BF),
            V((16, 256), BF),
            V((6, 16), jnp.int32),
            V((6, 16), F32),
            V((256, 2048), BF),
            V((1, 2048), F32),
            V((1, 2048), F32),
            V((2048, 256), BF),
            V((2048, 256), BF),
            V((256, 2048), BF),
            V((1, 2048), F32),
            V((16, 2048), BF),
            V((16, 2048), F32),
            V((16, 2048), F32),
            V((8, 16, 1024), BF),
            V((2, 16, 8, 1024), BF),
            V((2, 16, 8, 1024), BF),
            V((2, 16, 8, 1024), BF),
            V((2, 128, 1024), BF),
            V((2, 128, 1024), BF),
            V((2, 16, 8, 1024), BF),
            V((2, 16, 8, 1024), BF),
            V((8, 16, 1024), BF),
            V((8, 16, 1024), BF),
            V((16, 1024), F32),
            V((16, 2048), F32),
            V((16, 128), F32),
            V((8, 16, 128), F32),
            V((48, 128), BF),
            V((16, 48, 128), BF),
            V((8, 16, 256), BF),
            V((8, 16, 256), F32),
            V((8, 16, 256), F32),
            V((16, 128), BF),
            V((8, 16, 128), BF),
            V((8, 16, 256), F32),
            V((8, 16, 256), F32),
            V((8, 16, 256), F32),
            V((2, 128, 64), BF),
            V((2, 64, 128), BF),
            V((2, 64, 128), BF),
            dma((27,)),
            dma((96,)),
        ],
        compiler_params=pltpu.CompilerParams(
            collective_id=0, has_side_effects=True, vmem_limit_bytes=56 * 1024 * 1024
        ),
    )(
        tokens,
        norm_in.reshape(1, -1),
        w_query,
        w_key.T,
        w_value.T,
        cache_lengths,
        stick_bias,
        cache_keys.reshape(4, 256, 1024),
        cache_values.reshape(4, 256, 1024),
        dense_gate,
        dense_up,
        dense_down.T,
        routes.T,
        route_weights.T,
        w_output,
        norm_mid.reshape(1, -1),
        mix_gate.reshape(1, -1),
        expert_gate.reshape(2048, 256),
        expert_up.reshape(2048, 256),
        expert_down.reshape(256, 2048),
        norm_out.reshape(1, -1),
    )


def solution(mesh):
    split = Mesh(
        mesh.devices.reshape(NZ, NY, NX, mesh.shape["tp"]), ("ep_0", "ep_1", "ep_2", "tp")
    )
    return jax.shard_map(
        shards,
        mesh=split,
        in_specs=(
            P(EP, None),
            P(EP, "tp", None, None),
            P(EP, "tp", None, None),
            P(EP),
            P(),
            P(None, "tp"),
            P(None, "tp"),
            P(None, "tp"),
            P("tp"),
            P("tp", None),
            P(),
            P(EP, None),
            P(EP, None),
            P(EP, None, "tp"),
            P(EP, None, "tp"),
            P(EP, "tp", None),
            P(EP, None),
            P(EP, None),
            P(None, EP),
            P(),
            P(),
        ),
        out_specs=(P(EP, None), P(EP, "tp"), P(EP, "tp")),
        check_vma=False,
    )
```

```python
import jax
import jax.numpy as jnp
from jax import lax
from jax.experimental import pallas as pl
from jax.experimental.pallas import tpu as pltpu
from jax.sharding import Mesh
from jax.sharding import PartitionSpec as P

EP = ("ep_0", "ep_1", "ep_2")
MESH = pl.DeviceIdType.MESH
BF = jnp.bfloat16
F32 = jnp.float32
NZ, NY, NX = 8, 4, 4
PLANE = NY * NX
ORDER = (0, 4, 1, 7, 2, 6, 3, 5)
SLOT = {d: i for i, d in enumerate(ORDER)}
OFFS = sorted(
    ((dy, dx) for dy in range(NY) for dx in range(NX) if (dy, dx) != (0, 0)),
    key=lambda o: min(o[0], NY - o[0]) + min(o[1], NX - o[1]),
)
BACK = [OFFS.index(((-dy) % NY, (-dx) % NX)) for dy, dx in OFFS]
NP = len(OFFS)
NC = 4
HW = 1024 // NC


def dot(a, b):
    return jnp.dot(a, b, preferred_element_type=F32)


def dot_nt(a, b):
    return lax.dot_general(a, b, (((1,), (1,)), ((), ())), preferred_element_type=F32)


def rows(shape):
    return lax.broadcasted_iota(jnp.int32, shape, 0)


def cols(shape):
    return lax.broadcasted_iota(jnp.int32, shape, 1)


def ones_where(mask):
    return jnp.where(mask, 1.0, 0.0).astype(BF)


def norm(v, gain):
    center = jnp.mean(v, -1, keepdims=True)
    off = v - center
    spread = jnp.mean(off * off, -1, keepdims=True)
    return off * lax.rsqrt(spread + 1e-05) * gain


def halves(v):
    high = v.astype(BF)
    return high, (v - high.astype(F32)).astype(BF)


def body(
    tokens_h, norm_in_h, wq_h, wk_h, wv_h, lens_h, bias_h, ck, cv, dgate_h, dup_h, ddown_h,
    routes_h, weights_h, wo_h, norm_mid_h, mix_gate_h, eg_h, eu_h, ed_h, norm_out_h,
    out, fk, fv,
    tokens, norm_in, wq, wk, wv, lens, bias, kb, vb, dgate, dup, ddown,
    routes, weights, wo, norm_mid, mix_gate, eg, eu, ed, norm_out,
    egm, eum, edm, hb, pps, ppr, zb, ob, xb, eb, rb, fs, fb, fin,
    rts, rtb, dws, dwb, tb, d2s, d2b, das, dab, d4s, d4b, d4p,
    pm, wh, wl, ga,
    lsem, bank,
):
    z, y, x, c = (lax.axis_index(a) for a in (*EP, "tp"))
    me = y * NX + x
    o = 1 - c
    mate = (z, y, x, o)

    def along(d):
        return (lax.rem(z + d, NZ), y, x, c)

    def across(k):
        dy, dx = OFFS[k]
        return (z, lax.rem(y + dy, NY), lax.rem(x + dx, NX), c)

    def place(k):
        dy, dx = OFFS[k]
        return lax.rem(y + dy, NY) * NX + lax.rem(x + dx, NX)

    flags = {}

    def flag(*name):
        return bank.at[flags.setdefault(name, len(flags))]

    def send(src, dst, out_flag, in_flag, dev):
        pltpu.make_async_remote_copy(
            src_ref=src, dst_ref=dst, send_sem=out_flag, recv_sem=in_flag,
            device_id=dev, device_id_type=MESH,
        ).start()

    def await_bytes(ref, name):
        pltpu.make_async_copy(ref, ref, name).wait()

    reads = {}

    def fetch(name, src, dst):
        copy = pltpu.make_async_copy(src, dst, lsem.at[len(reads)])
        copy.start()
        reads[name] = copy

    def ready(*names):
        for name in names:
            reads[name].wait()

    fetch("tokens", tokens_h, tokens)
    fetch("norm_in", norm_in_h, norm_in)
    fetch("wq", wq_h, wq)
    fetch("wk", wk_h, wk)
    fetch("wv", wv_h, wv)
    fetch("dgate", dgate_h, dgate)
    fetch("dup", dup_h, dup)
    fetch("ddown", ddown_h, ddown)
    fetch("routes", routes_h, routes)
    fetch("weights", weights_h, weights)
    for b in range(4):
        fetch(("k", b), ck.at[b], kb.at[b])
    fetch("lens", lens_h, lens)
    fetch("bias", bias_h, bias)
    for b in range(4):
        fetch(("v", b), cv.at[b], vb.at[b])
    fetch("wo", wo_h, wo)
    fetch("norm_mid", norm_mid_h, norm_mid)
    fetch("mix_gate", mix_gate_h, mix_gate)

    barrier = pltpu.get_barrier_semaphore()
    for d in range(1, NZ):
        pl.semaphore_signal(barrier, inc=1, device_id=along(d), device_id_type=MESH)
    for k in range(NP):
        pl.semaphore_signal(barrier, inc=1, device_id=across(k), device_id_type=MESH)
    pl.semaphore_signal(barrier, inc=1, device_id=mate, device_id_type=MESH)

    ready("tokens", "norm_in")
    normed = norm(tokens[...].astype(F32), norm_in[...]).astype(BF)
    ready("wq", "wk", "wv")
    queries = dot(normed, wq[...]).astype(BF)
    fk[...] = dot_nt(normed, wk[...]).astype(BF)
    fv[...] = dot_nt(normed, wv[...]).astype(BF)

    half = pl.ds(pl.multiple_of(c * 128, 128), 128)
    ready("dgate", "dup", "ddown", "routes", "weights")
    dws[0:16] = dgate[:, half]
    dws[16:32] = dup[:, half]
    dws[32:48] = ddown[:, half]
    rts[...] = jnp.zeros((16, 128), F32)
    for j in range(8):
        rts[0:6, 16 * j : 16 * j + 16] = routes[...].astype(F32)
        rts[8:14, 16 * j : 16 * j + 16] = weights[...]

    pl.semaphore_wait(barrier, NZ - 1 + NP + 1)
    for k in range(NP):
        send(dws, dwb.at[me], flag("ws"), flag("wr"), across(k))
    for d in ORDER[1:]:
        send(rts, rtb.at[SLOT[NZ - d]], flag("ts"), flag("tr"), along(d))
    dwb[me] = dws[...]
    rtb[0] = rts[...]

    wide = (64, 256)
    expand = ones_where(rows((64, 16)) // 4 == cols((64, 16)))
    fold = ones_where(lax.rem(rows((256, 256)), 64) == lax.rem(cols((256, 256)), 64))
    head_of = cols(wide) // 64 == lax.rem(rows(wide), 4)
    seq_of = cols(wide) // 64 == lax.rem(rows(wide) // 4, 4)
    picked = jnp.where(head_of, dot(expand, queries), 0.0).astype(BF)
    grid = jnp.where(seq_of, dot(picked, fold), 0.0).astype(BF)
    parts = []
    ready(*(("k", b) for b in range(4)))
    for b in range(4):
        parts.append(dot(grid[16 * b : 16 * b + 16], kb[b]))
    scores = jnp.concatenate(parts, axis=0) * 0.125
    ready("lens", "bias")
    row = rows((64, 128))
    length = jnp.zeros((64, 128), jnp.int32)
    for s in range(16):
        length = jnp.where(row // 4 == s, lens[s], length)
    offset = jnp.zeros((64, 128), F32)
    for g in range(4):
        offset = jnp.where(lax.rem(row, 4) == g, bias[g], offset)
    later = ones_where(rows((128, 128)) >= cols((128, 128)))
    zs, keeps, seen = [], [], []
    for n in range(8):
        zn = scores[:, 128 * n : 128 * n + 128] + offset
        vis = cols((64, 128)) + 128 * n < length
        soft = jnp.maximum(zn, 0.0) + jnp.log1p(jnp.exp(-jnp.abs(zn)))
        zs.append(zn)
        seen.append(vis)
        keeps.append(jnp.where(vis, soft, 0.0))
    high, low = halves(jnp.concatenate(keeps, axis=0))
    within = dot(high, later) + dot(low, later)
    carry = jnp.zeros((64, 1), F32)
    sticks = [None] * 8
    for n in range(7, -1, -1):
        w = within[64 * n : 64 * n + 64]
        sticks[n] = jnp.where(seen[n], jnp.exp(zs[n] - w - carry), 0.0).astype(BF)
        carry = carry + w[:, 0:1]
    stick = jnp.concatenate(sticks, axis=1)
    parts = []
    ready(*(("v", b) for b in range(4)))
    fetch("eg", eg_h, eg)
    fetch("eu", eu_h, eu)
    fetch("ed", ed_h, ed)
    fetch("norm_out", norm_out_h, norm_out)
    for b in range(4):
        parts.append(dot_nt(stick[16 * b : 16 * b + 16], vb[b]))
    att = jnp.where(seq_of, jnp.concatenate(parts, axis=0), 0.0).astype(BF)
    att = jnp.where(head_of, dot(att, fold), 0.0).astype(BF)
    gather = ones_where(cols((16, 64)) // 4 == rows((16, 64)))
    attended = dot(gather, att).astype(BF)
    ready("wo")
    pps[...] = dot(attended, wo[...])
    send(pps, ppr, flag("ps"), flag("pr"), mate)

    await_bytes(rtb.at[1:8], flag("tr"))
    shape = (128, 64)
    expert = (z * PLANE + rows(shape) // 8).astype(F32)
    ahead = ones_where(
        (rows((64, 64)) < cols((64, 64))) & (rows((64, 64)) // 16 == cols((64, 64)) // 16)
    )
    table = jnp.zeros((16, 64), F32)
    for j in range(4):
        table = jnp.where(cols((16, 64)) // 16 == j, rtb[4 * c + j][:, 0:64], table)
    hit = jnp.zeros(shape, F32)
    share = jnp.zeros(shape, F32)
    for k in range(6):
        same = table[k : k + 1] == expert
        hit = jnp.where(same, 1.0, hit)
        share = jnp.where(same, table[8 + k : 9 + k], share)
    rank = dot(hit.astype(BF), ahead)
    here = (
        (hit > 0.5)
        & (rank == lax.rem(rows(shape), 2).astype(F32))
        & (cols(shape) // 16 == lax.rem(rows(shape), 8) // 2)
    )
    pm[...] = ones_where(here)
    wh[...], wl[...] = halves(jnp.transpose(jnp.where(here, share, 0.0)))
    await_bytes(rtb.at[1:8], flag("ts"))
    await_bytes(dwb.at[0:15], flag("ws"))

    own_half = pl.ds(pl.multiple_of(c * 1024, 1024), 1024)
    mate_half = pl.ds(pl.multiple_of(o * 1024, 1024), 1024)
    ready("norm_mid", "mix_gate")
    await_bytes(ppr, flag("pr"))
    hidden = norm(normed.astype(F32) + (pps[...] + ppr[...]), norm_mid[...]).astype(BF)
    hb[...] = hidden
    for f in range(NC):
        source = hb.at[:, pl.ds(pl.multiple_of(c * 1024 + f * HW, HW), HW)]
        lanes = pl.ds(pl.multiple_of(c * HW, HW), HW)
        for d in (4, 1, 7, 3, 5, 2, 6):
            t = SLOT[NZ - d]
            there = (lax.rem(z + d, NZ), y, x, t // 4)
            send(source, zb.at[f, t % 4, :, lanes], flag("zs"), flag("zr", f), there)

    @pl.when(c == 0)
    def _():
        for f in range(NC):
            for h in range(2):
                at = 1024 * h + HW * f
                zb[f, 0, :, HW * h : HW * h + HW] = hb[:, at : at + HW]

    mixing = jax.nn.sigmoid(jnp.sum(hidden.astype(F32) * mix_gate[...], -1, keepdims=True))
    await_bytes(pps, flag("ps"))
    ready("eg", "eu", "ed")
    send(eg, egm, flag("g0s"), flag("g0r"), mate)
    send(eu, eum, flag("g1s"), flag("g1r"), mate)
    send(ed, edm, flag("g2s"), flag("g2r"), mate)

    for f in range(NC):

        @pl.when(c == 0)
        def _():
            await_bytes(zb.at[f, 1:4], flag("zr", f))

        @pl.when(c == 1)
        def _():
            await_bytes(zb.at[f], flag("zr", f))

        going = dot(pm[...], zb[f].reshape(64, 2 * HW))
        for q in range(PLANE):
            ob[f, q] = going[8 * q : 8 * q + 8].astype(BF)
        for k in range(NP):
            send(ob.at[f, place(k)], xb.at[f, me], flag("xs", f), flag("xr", f), across(k))
        xb[f, me] = ob[f, me]

    inner = lax.rem(z, 4) * 256
    chunk = inner // HW
    features = pl.ds(pl.multiple_of((z // 4) * HW + lax.rem(inner, HW), 256), 256)
    own_group = pl.ds(4 * c, 4)
    mate_group = pl.ds(4 * o, 4)
    send(zb.at[chunk, :, :, features], tb.at[own_group], flag("cs"), flag("cr"), mate)
    tb[own_group] = zb[chunk, :, :, features]
    await_bytes(dwb.at[0:15], flag("wr"))
    await_bytes(tb.at[mate_group], flag("cr"))
    column = tb[...].reshape(128, 256)
    pre = dot(column, dwb[:, 0:16, :].reshape(256, 128))
    lin = dot(column, dwb[:, 16:32, :].reshape(256, 128))
    for s in range(NZ):
        d2s[s, :, 0:128] = pre[16 * s : 16 * s + 16].astype(BF)
        d2s[s, :, 128:256] = lin[16 * s : 16 * s + 16].astype(BF)
    for d in ORDER[1:]:
        send(d2s.at[SLOT[d]], d2b.at[SLOT[NZ - d]], flag("d2s"), flag("d2r"), along(d))
    d2b[0] = d2s[0]
    await_bytes(tb.at[own_group], flag("cs"))
    await_bytes(fb.at[:, 1:8], flag("zs"))
    await_bytes(egm, flag("g0s"))
    await_bytes(eum, flag("g1s"))
    await_bytes(edm, flag("g2s"))
    await_bytes(egm, flag("g0r"))
    await_bytes(eum, flag("g1r"))
    await_bytes(edm, flag("g2r"))

    sums = [None] * 4
    for f in range(NC):
        await_bytes(xb.at[f, 0:15], flag("xr", f))
        arrived = xb[f].reshape(128, 2 * HW)
        for i, ref in enumerate((eg, eu, egm, eum)):
            step = dot(arrived[:, 0:HW], ref[HW * f : HW * f + HW])
            step = step + dot(arrived[:, HW : 2 * HW], ref[1024 + HW * f : 1024 + HW * f + HW])
            if f > 0:
                step = step + ga[i]
            if f < NC - 1:
                ga[i] = step
            sums[i] = step
    acts = [(jax.nn.silu(sums[i]) * sums[i + 1]).astype(BF) for i in (0, 2)]
    for f in range(NC):
        for h in range(2):
            at = 1024 * h + HW * f
            total = dot(acts[0], ed[:, at : at + HW]).astype(BF).astype(F32)
            total = total + dot(acts[1], edm[:, at : at + HW]).astype(BF).astype(F32)
            for q in range(PLANE):
                eb[f, q, :, HW * h : HW * h + HW] = total[8 * q : 8 * q + 8].astype(BF)
        for k in range(NP):
            send(eb.at[f, place(k)], rb.at[f, me], flag("es", f), flag("er", f), across(k))
        rb[f, me] = eb[f, me]
    for f in range(NC):
        await_bytes(xb.at[f, 0:15], flag("xs", f))

    await_bytes(d2b.at[1:8], flag("d2r"))
    summed = jnp.sum(d2b[...].astype(F32), axis=0)
    das[...] = (jax.nn.silu(summed[:, 0:128]) * summed[:, 128:256]).astype(BF)
    for d in ORDER[1:]:
        send(das, dab.at[SLOT[NZ - d]], flag("d3s"), flag("d3r"), along(d))
    dab[0] = das[...]
    await_bytes(d2b.at[1:8], flag("d2s"))

    def combine(f, group):
        await_bytes(rb.at[f, 0:15], flag("er", f))
        block = rb[f].reshape(128, 2 * HW)
        part = dot(wh[...], block) + dot(wl[...], block)
        for j in range(4):
            d = ORDER[4 * group + j]
            fs[f, j] = part[16 * j : 16 * j + 16].astype(BF)
            if d == 0:
                send(fs.at[f, j, :, HW : 2 * HW], fb.at[f, 0], flag("fs"), flag("fr", f), mate)
                fb[f, 0] = fs[f, j, :, 0:HW]
                continue
            for h in range(2):
                there = (lax.rem(z + d, NZ), y, x, h)
                piece = fs.at[f, j, :, HW * h : HW * h + HW]
                send(piece, fb.at[f, SLOT[NZ - d]], flag("fs"), flag("fr", f), there)
        await_bytes(rb.at[f, 0:15], flag("es", f))

    for f in range(NC):
        pl.when(c == 0)(lambda: combine(f, 0))
        pl.when(c == 1)(lambda: combine(f, 1))
        if f == 0:
            await_bytes(dab.at[1:8], flag("d3r"))
            block = dot_nt(dab[...].reshape(128, 128), dwb[:, 32:48, :].reshape(256, 128))
            for s in range(NZ):
                d4s[s] = block[16 * s : 16 * s + 16].astype(BF)
            for d in ORDER[1:]:
                send(d4s.at[SLOT[d]], d4b.at[z], flag("d4s"), flag("d4r"), along(d))
            d4b[z] = d4s[0]
            await_bytes(dab.at[1:8], flag("d3s"))

    await_bytes(d4b.at[0:7], flag("d4r"))
    send(d4b, d4p, flag("d5s"), flag("d5r"), mate)
    ready("norm_out")
    await_bytes(d4b.at[0:7], flag("d4s"))

    for f in range(NC):

        @pl.when(c == 0)
        def _():
            await_bytes(fb.at[f, 1:8], flag("fr", f))

        @pl.when(c == 1)
        def _():
            await_bytes(fb.at[f], flag("fr", f))

        piece = pl.ds(pl.multiple_of(c * 1024 + HW * f, HW), HW)
        fin[:, piece] = jnp.sum(fb[f].astype(F32), axis=0)
        send(fin.at[:, piece], fin.at[:, piece], flag("us"), flag("ur"), mate)
        if f == 0:
            await_bytes(d4p, flag("d5r"))
            mixed = hidden.astype(F32) + mixing * jnp.concatenate(
                [d4b[n].astype(F32) + d4p[n].astype(F32) for n in range(NZ)], axis=1
            )
            await_bytes(d4p, flag("d5s"))

    @pl.when(c == 0)
    def _():
        await_bytes(fb.at[:, 0:7], flag("fs"))

    @pl.when(c == 1)
    def _():
        await_bytes(fb, flag("fs"))

    await_bytes(fin.at[:, mate_half], flag("ur"))
    out[...] = norm(mixed + fin[...], norm_out[...]).astype(BF)
    await_bytes(fin.at[:, own_half], flag("us"))


def shards(
    tokens, cache_keys, cache_values, cache_lengths, norm_in, w_query, w_key, w_value,
    stick_bias, w_output, norm_mid, routes, route_weights, expert_gate, expert_up,
    expert_down, dense_gate, dense_up, dense_down, mix_gate, norm_out,
):
    vmem = pl.BlockSpec(memory_space=pltpu.VMEM)
    hbm = pl.BlockSpec(memory_space=pltpu.HBM)
    dma = pltpu.SemaphoreType.DMA
    V = pltpu.VMEM
    return pl.pallas_call(
        body,
        out_shape=(V((16, 2048), BF), V((16, 64), BF), V((16, 64), BF)),
        in_specs=[hbm] * 21,
        out_specs=(vmem, vmem, vmem),
        scratch_shapes=[
            V((16, 2048), BF),
            V((1, 2048), F32),
            V((2048, 256), BF),
            V((64, 2048), BF),
            V((64, 2048), BF),
            pltpu.SMEM((16,), jnp.int32),
            pltpu.SMEM((4,), F32),
            V((4, 256, 1024), BF),
            V((4, 256, 1024), BF),
            V((16, 256), BF),
            V((16, 256), BF),
            V((16, 256), BF),
            V((6, 16), jnp.int32),
            V((6, 16), F32),
            V((256, 2048), BF),
            V((1, 2048), F32),
            V((1, 2048), F32),
            V((2048, 256), BF),
            V((2048, 256), BF),
            V((256, 2048), BF),
            V((1, 2048), F32),
            V((2048, 256), BF),
            V((2048, 256), BF),
            V((256, 2048), BF),
            V((16, 2048), BF),
            V((16, 2048), F32),
            V((16, 2048), F32),
            V((NC, 4, 16, 2 * HW), BF),
            V((NC, 16, 8, 2 * HW), BF),
            V((NC, 16, 8, 2 * HW), BF),
            V((NC, 16, 8, 2 * HW), BF),
            V((NC, 16, 8, 2 * HW), BF),
            V((NC, 4, 16, 2 * HW), BF),
            V((NC, 8, 16, HW), BF),
            V((16, 2048), F32),
            V((16, 128), F32),
            V((8, 16, 128), F32),
            V((48, 128), BF),
            V((16, 48, 128), BF),
            V((8, 16, 256), BF),
            V((8, 16, 256), BF),
            V((8, 16, 256), BF),
            V((16, 128), BF),
            V((8, 16, 128), BF),
            V((8, 16, 256), BF),
            V((8, 16, 256), BF),
            V((8, 16, 256), BF),
            V((128, 64), BF),
            V((64, 128), BF),
            V((64, 128), BF),
            V((4, 128, 256), F32),
            dma((27,)),
            dma((96,)),
        ],
        compiler_params=pltpu.CompilerParams(
            collective_id=0, has_side_effects=True, vmem_limit_bytes=56 * 1024 * 1024
        ),
    )(
        tokens,
        norm_in.reshape(1, -1),
        w_query,
        w_key.T,
        w_value.T,
        cache_lengths,
        stick_bias,
        cache_keys.reshape(4, 256, 1024),
        cache_values.reshape(4, 256, 1024),
        dense_gate,
        dense_up,
        dense_down.T,
        routes.T,
        route_weights.T,
        w_output,
        norm_mid.reshape(1, -1),
        mix_gate.reshape(1, -1),
        expert_gate.reshape(2048, 256),
        expert_up.reshape(2048, 256),
        expert_down.reshape(256, 2048),
        norm_out.reshape(1, -1),
    )


def solution(mesh):
    split = Mesh(
        mesh.devices.reshape(NZ, NY, NX, mesh.shape["tp"]), ("ep_0", "ep_1", "ep_2", "tp")
    )
    return jax.shard_map(
        shards,
        mesh=split,
        in_specs=(
            P(EP, None),
            P(EP, "tp", None, None),
            P(EP, "tp", None, None),
            P(EP),
            P(),
            P(None, "tp"),
            P(None, "tp"),
            P(None, "tp"),
            P("tp"),
            P("tp", None),
            P(),
            P(EP, None),
            P(EP, None),
            P(EP, None, "tp"),
            P(EP, None, "tp"),
            P(EP, "tp", None),
            P(EP, None),
            P(EP, None),
            P(None, EP),
            P(),
            P(),
        ),
        out_specs=(P(EP, None), P(EP, "tp"), P(EP, "tp")),
        check_vma=False,
    )
```

```python
import jax
import jax.numpy as jnp
from jax import lax
from jax.experimental import pallas as pl
from jax.experimental.pallas import tpu as pltpu
from jax.sharding import Mesh
from jax.sharding import PartitionSpec as P

EP = ("ep_0", "ep_1", "ep_2")
MESH = pl.DeviceIdType.MESH
BF = jnp.bfloat16
F32 = jnp.float32
NZ, NY, NX = 8, 4, 4
PLANE = NY * NX
ORDER = (0, 1, 7, 2, 6, 3, 5, 4)
SLOT = {d: i for i, d in enumerate(ORDER)}
OFFS = sorted(
    ((dy, dx) for dy in range(NY) for dx in range(NX) if (dy, dx) != (0, 0)),
    key=lambda o: -min(o[0], NY - o[0]) - min(o[1], NX - o[1]),
)
BACK = [OFFS.index(((-dy) % NY, (-dx) % NX)) for dy, dx in OFFS]
NP = len(OFFS)
NC = 4
HW = 1024 // NC


def dot(a, b):
    return jnp.dot(a, b, preferred_element_type=F32)


def dot_nt(a, b):
    return lax.dot_general(a, b, (((1,), (1,)), ((), ())), preferred_element_type=F32)


def rows(shape):
    return lax.broadcasted_iota(jnp.int32, shape, 0)


def cols(shape):
    return lax.broadcasted_iota(jnp.int32, shape, 1)


def ones_where(mask):
    return jnp.where(mask, 1.0, 0.0).astype(BF)


def norm(v, gain):
    center = jnp.mean(v, -1, keepdims=True)
    off = v - center
    spread = jnp.mean(off * off, -1, keepdims=True)
    return off * lax.rsqrt(spread + 1e-05) * gain


def halves(v):
    high = v.astype(BF)
    return high, (v - high.astype(F32)).astype(BF)


def body(
    tokens_h, norm_in_h, wq_h, wk_h, wv_h, lens_h, bias_h, ck, cv, dgate_h, dup_h, ddown_h,
    routes_h, weights_h, wo_h, norm_mid_h, mix_gate_h, eg_h, eu_h, ed_h, norm_out_h,
    res,
    tokens, norm_in, wq, wk, wv, lens, bias, kb, vb, dgate, dup, ddown,
    routes, weights, wo, norm_mid, mix_gate, eg, eu, ed, norm_out,
    egm, eum, edm, hb, pps, ppr, zb, ob, xb, eb, rb, fs, fb, fin,
    rts, rtb, dws, dwb, d2s, d2b, das, dab, d3m, d4s, d4b,
    pm, wh, wl, ga,
    lsem, bank,
):
    out, fk, fv = res.at[:, 0:2048], res.at[:, 2048:2112], res.at[:, 2176:2240]
    z, y, x, c = (lax.axis_index(a) for a in (*EP, "tp"))
    me = y * NX + x
    o = 1 - c
    mate = (z, y, x, o)

    def along(d):
        return (lax.rem(z + d, NZ), y, x, c)

    def across(k):
        dy, dx = OFFS[k]
        return (z, lax.rem(y + dy, NY), lax.rem(x + dx, NX), c)

    def place(k):
        dy, dx = OFFS[k]
        return lax.rem(y + dy, NY) * NX + lax.rem(x + dx, NX)

    flags = {}

    def flag(*name):
        return bank.at[flags.setdefault(name, len(flags))]

    def send(src, dst, out_flag, in_flag, dev):
        pltpu.make_async_remote_copy(
            src_ref=src, dst_ref=dst, send_sem=out_flag, recv_sem=in_flag,
            device_id=dev, device_id_type=MESH,
        ).start()

    def await_bytes(ref, name):
        pltpu.make_async_copy(ref, ref, name).wait()

    reads = {}

    def fetch(name, src, dst):
        copy = pltpu.make_async_copy(src, dst, lsem.at[len(reads)])
        copy.start()
        reads[name] = copy

    def ready(*names):
        for name in names:
            reads[name].wait()

    fetch("tokens", tokens_h, tokens)
    fetch("norm_in", norm_in_h, norm_in)
    fetch("wq", wq_h, wq)
    fetch("wk", wk_h, wk)
    fetch("wv", wv_h, wv)
    fetch("dgate", dgate_h, dgate)
    fetch("dup", dup_h, dup)
    fetch("ddown", ddown_h, ddown)
    fetch("routes", routes_h, routes)
    fetch("weights", weights_h, weights)
    for b in range(4):
        fetch(("k", b), ck.at[b], kb.at[b])
    fetch("lens", lens_h, lens)
    fetch("bias", bias_h, bias)
    for b in range(4):
        fetch(("v", b), cv.at[b], vb.at[b])
    fetch("wo", wo_h, wo)
    fetch("norm_mid", norm_mid_h, norm_mid)
    fetch("mix_gate", mix_gate_h, mix_gate)

    barrier = pltpu.get_barrier_semaphore()
    for d in range(1, NZ):
        pl.semaphore_signal(barrier, inc=1, device_id=along(d), device_id_type=MESH)
    for k in range(NP):
        pl.semaphore_signal(barrier, inc=1, device_id=across(k), device_id_type=MESH)
    pl.semaphore_signal(barrier, inc=1, device_id=mate, device_id_type=MESH)

    ready("tokens", "norm_in")
    normed = norm(tokens[...].astype(F32), norm_in[...]).astype(BF)
    ready("wq", "wk", "wv")
    queries = dot(normed, wq[...]).astype(BF)
    fk[...] = dot_nt(normed, wk[...]).astype(BF)
    fv[...] = dot_nt(normed, wv[...]).astype(BF)

    ready("dgate", "dup", "ddown", "routes", "weights")
    dws[0:16] = dgate[...]
    dws[16:32] = dup[...]
    dws[32:48] = ddown[...]
    rts[...] = jnp.zeros((16, 128), F32)
    for j in range(8):
        rts[0:6, 16 * j : 16 * j + 16] = routes[...].astype(F32)
        rts[8:14, 16 * j : 16 * j + 16] = weights[...]

    pl.semaphore_wait(barrier, NZ - 1 + NP + 1)
    for k in range(NP):
        send(dws, dwb.at[me], flag("ws"), flag("wr"), across(k))
    for d in ORDER[1:]:
        send(rts, rtb.at[SLOT[NZ - d]], flag("ts"), flag("tr"), along(d))
    dwb[me] = dws[...]
    rtb[0] = rts[...]

    wide = (64, 256)
    expand = ones_where(rows((64, 16)) // 4 == cols((64, 16)))
    fold = ones_where(lax.rem(rows((256, 256)), 64) == lax.rem(cols((256, 256)), 64))
    head_of = cols(wide) // 64 == lax.rem(rows(wide), 4)
    seq_of = cols(wide) // 64 == lax.rem(rows(wide) // 4, 4)
    picked = jnp.where(head_of, dot(expand, queries), 0.0).astype(BF)
    grid = jnp.where(seq_of, dot(picked, fold), 0.0).astype(BF)
    parts = []
    ready(*(("k", b) for b in range(4)))
    for b in range(4):
        parts.append(dot(grid[16 * b : 16 * b + 16], kb[b]))
    scores = jnp.concatenate(parts, axis=0) * 0.125
    ready("lens", "bias")
    row = rows((64, 128))
    length = jnp.zeros((64, 128), jnp.int32)
    for s in range(16):
        length = jnp.where(row // 4 == s, lens[s], length)
    offset = jnp.zeros((64, 128), F32)
    for g in range(4):
        offset = jnp.where(lax.rem(row, 4) == g, bias[g], offset)
    later = ones_where(rows((128, 128)) >= cols((128, 128)))
    zs, keeps, seen = [], [], []
    for n in range(8):
        zn = scores[:, 128 * n : 128 * n + 128] + offset
        vis = cols((64, 128)) + 128 * n < length
        soft = jnp.maximum(zn, 0.0) + jnp.log1p(jnp.exp(-jnp.abs(zn)))
        zs.append(zn)
        seen.append(vis)
        keeps.append(jnp.where(vis, soft, 0.0))
    high, low = halves(jnp.concatenate(keeps, axis=0))
    within = dot(high, later) + dot(low, later)
    carry = jnp.zeros((64, 1), F32)
    sticks = [None] * 8
    for n in range(7, -1, -1):
        w = within[64 * n : 64 * n + 64]
        sticks[n] = jnp.where(seen[n], jnp.exp(zs[n] - w - carry), 0.0).astype(BF)
        carry = carry + w[:, 0:1]
    stick = jnp.concatenate(sticks, axis=1)
    parts = []
    ready(*(("v", b) for b in range(4)))
    fetch("eg", eg_h, eg)
    fetch("eu", eu_h, eu)
    fetch("ed", ed_h, ed)
    fetch("norm_out", norm_out_h, norm_out)
    for b in range(4):
        parts.append(dot_nt(stick[16 * b : 16 * b + 16], vb[b]))
    att = jnp.where(seq_of, jnp.concatenate(parts, axis=0), 0.0).astype(BF)
    att = jnp.where(head_of, dot(att, fold), 0.0).astype(BF)
    gather = ones_where(cols((16, 64)) // 4 == rows((16, 64)))
    attended = dot(gather, att).astype(BF)
    ready("wo")
    pps[...] = dot(attended, wo[...])
    send(pps, ppr, flag("ps"), flag("pr"), mate)

    await_bytes(rtb.at[1:8], flag("tr"))
    shape = (128, 64)
    expert = (z * PLANE + rows(shape) // 8).astype(F32)
    ahead = ones_where(
        (rows((64, 64)) < cols((64, 64))) & (rows((64, 64)) // 16 == cols((64, 64)) // 16)
    )
    table = jnp.zeros((16, 64), F32)
    for j in range(4):
        table = jnp.where(cols((16, 64)) // 16 == j, rtb[4 * c + j][:, 0:64], table)
    hit = jnp.zeros(shape, F32)
    share = jnp.zeros(shape, F32)
    for k in range(6):
        same = table[k : k + 1] == expert
        hit = jnp.where(same, 1.0, hit)
        share = jnp.where(same, table[8 + k : 9 + k], share)
    rank = dot(hit.astype(BF), ahead)
    here = (
        (hit > 0.5)
        & (rank == lax.rem(rows(shape), 2).astype(F32))
        & (cols(shape) // 16 == lax.rem(rows(shape), 8) // 2)
    )
    pm[...] = ones_where(here)
    wh[...], wl[...] = halves(jnp.transpose(jnp.where(here, share, 0.0)))
    await_bytes(rtb.at[1:8], flag("ts"))
    await_bytes(dwb.at[0:15], flag("ws"))

    own_half = pl.ds(pl.multiple_of(c * 1024, 1024), 1024)
    mate_half = pl.ds(pl.multiple_of(o * 1024, 1024), 1024)
    ready("norm_mid", "mix_gate")
    await_bytes(ppr, flag("pr"))
    hidden = norm(normed.astype(F32) + (pps[...] + ppr[...]), norm_mid[...]).astype(BF)
    hb[...] = hidden
    lanes = pl.ds(pl.multiple_of(c * HW, HW), HW)
    for f, d in [(f, d) for f in range(NC) for d in (4, 3, 5, 2, 6, 1, 7)]:
        source = hb.at[:, pl.ds(pl.multiple_of(c * 1024 + f * HW, HW), HW)]
        t = SLOT[NZ - d]
        there = (lax.rem(z + d, NZ), y, x, t // 4)
        send(source, zb.at[f, t % 4, :, lanes], flag("zs"), flag("zr", f), there)

    @pl.when(c == 0)
    def _():
        for f in range(NC):
            for h in range(2):
                at = 1024 * h + HW * f
                zb[f, 0, :, HW * h : HW * h + HW] = hb[:, at : at + HW]

    mixing = jax.nn.sigmoid(jnp.sum(hidden.astype(F32) * mix_gate[...], -1, keepdims=True))
    await_bytes(pps, flag("ps"))
    ready("eg", "eu", "ed")
    send(eg, egm, flag("g0s"), flag("g0r"), mate)
    send(eu, eum, flag("g1s"), flag("g1r"), mate)
    send(ed, edm, flag("g2s"), flag("g2r"), mate)

    for f in range(NC):

        @pl.when(c == 0)
        def _():
            await_bytes(zb.at[f, 1:4], flag("zr", f))

        @pl.when(c == 1)
        def _():
            await_bytes(zb.at[f], flag("zr", f))

        going = dot(pm[...], zb[f].reshape(64, 2 * HW))
        for q in range(PLANE):
            ob[f, q] = going[8 * q : 8 * q + 8].astype(BF)
        for k in range(NP):
            send(ob.at[f, place(k)], xb.at[f, me], flag("xs", f), flag("xr", f), across(k))
        xb[f, me] = ob[f, me]

    inner = lax.rem(z, 4) * 256
    features = pl.ds(pl.multiple_of((z // 4) * HW + lax.rem(inner, HW), 256), 256)
    column = zb[inner // HW, :, :, features].reshape(64, 256)
    await_bytes(dwb.at[0:15], flag("wr"))
    pre = dot(column, dwb[:, 0:16, :].reshape(256, 256))
    lin = dot(column, dwb[:, 16:32, :].reshape(256, 256))
    for j in range(4):
        for h in range(2):
            for i, v in enumerate((pre, lin)):
                at = 256 * h + 128 * i
                d2s[j, :, at : at + 128] = v[16 * j : 16 * j + 16, 128 * h : 128 * h + 128].astype(BF)

    def to_owners(group, source, target, name, width, f):
        for j in range(4):
            d = ORDER[4 * group + j]
            for h in range(2):
                piece = source.at[j, :, width * h : width * h + width]
                slot = target.at[SLOT[(NZ - d) % NZ]]
                if d:
                    there = (lax.rem(z + d, NZ), y, x, h)
                elif h:
                    there = mate
                else:
                    target[0] = source[j, :, 0:width]
                    continue
                send(piece, slot, flag(name, "s"), flag(name, "r", f), there)

    pl.when(c == 0)(lambda: to_owners(0, d2s, d2b, "d2", 256, 0))
    pl.when(c == 1)(lambda: to_owners(1, d2s, d2b, "d2", 256, 0))
    await_bytes(fb.at[:, 1:8], flag("zs"))
    await_bytes(egm, flag("g0s"))
    await_bytes(eum, flag("g1s"))
    await_bytes(edm, flag("g2s"))
    await_bytes(egm, flag("g0r"))
    await_bytes(eum, flag("g1r"))
    await_bytes(edm, flag("g2r"))

    sums = [None] * 4
    for f in range(NC):
        await_bytes(xb.at[f, 0:15], flag("xr", f))
        arrived = xb[f].reshape(128, 2 * HW)
        for i, ref in enumerate((eg, eu, egm, eum)):
            step = dot(arrived[:, 0:HW], ref[HW * f : HW * f + HW])
            step = step + dot(arrived[:, HW : 2 * HW], ref[1024 + HW * f : 1024 + HW * f + HW])
            if f > 0:
                step = step + ga[i]
            if f < NC - 1:
                ga[i] = step
            sums[i] = step
    acts = [(jax.nn.silu(sums[i]) * sums[i + 1]).astype(BF) for i in (0, 2)]
    for f in range(NC):
        for h in range(2):
            at = 1024 * h + HW * f
            total = dot(acts[0], ed[:, at : at + HW]).astype(BF).astype(F32)
            total = total + dot(acts[1], edm[:, at : at + HW]).astype(BF).astype(F32)
            for q in range(PLANE):
                eb[f, q, :, HW * h : HW * h + HW] = total[8 * q : 8 * q + 8].astype(BF)
        for k in range(NP):
            send(eb.at[f, place(k)], rb.at[f, me], flag("es", f), flag("er", f), across(k))
        rb[f, me] = eb[f, me]
    for f in range(NC):
        await_bytes(xb.at[f, 0:15], flag("xs", f))

    @pl.when(c == 0)
    def _():
        await_bytes(d2b.at[1:8], flag("d2", "r", 0))
        await_bytes(d2b.at[1:8], flag("d2", "s"))

    @pl.when(c == 1)
    def _():
        await_bytes(d2b, flag("d2", "r", 0))
        await_bytes(d2b, flag("d2", "s"))

    summed = jnp.sum(d2b[...].astype(F32), axis=0)
    das[...] = (jax.nn.silu(summed[:, 0:128]) * summed[:, 128:256]).astype(BF)
    lanes = pl.ds(pl.multiple_of(c * 128, 128), 128)
    for d in ORDER[1:]:
        t = SLOT[NZ - d]
        there = (lax.rem(z + d, NZ), y, x, t // 4)
        send(das, dab.at[t % 4, :, lanes], flag("d3s"), flag("d3r"), there)

    @pl.when(c == 0)
    def _():
        dab[0, :, 0:128] = das[...]

    @pl.when(c == 1)
    def _():
        send(das, dab.at[0, :, 128:256], flag("d3s"), flag("d3r"), mate)

    def dense_columns(group):
        if group == 0:
            await_bytes(d3m.at[0:7], flag("d3r"))
            await_bytes(d3m.at[0:7], flag("d3s"))
        else:
            await_bytes(d3m, flag("d3r"))
            await_bytes(d3m, flag("d3s"))
        block = dot_nt(dab[...].reshape(64, 256), dwb[:, 32:48, :].reshape(256, 256))
        spot = lax.rem(z, 4)
        for j in range(4):
            d = ORDER[4 * group + j]
            d4s[j] = block[16 * j : 16 * j + 16].astype(BF)
            if d:
                there = (lax.rem(z + d, NZ), y, x, z // 4)
                send(d4s.at[j], d4b.at[spot], flag("d4s"), flag("d4r"), there)
                continue

            @pl.when(z < 4)
            def _():
                d4b[spot] = d4s[j]

            @pl.when(z >= 4)
            def _():
                send(d4s.at[j], d4b.at[spot], flag("d4s"), flag("d4r"), mate)

    def combine(f, group):
        await_bytes(rb.at[f, 0:15], flag("er", f))
        block = rb[f].reshape(128, 2 * HW)
        part = dot(wh[...], block) + dot(wl[...], block)
        for j in range(4):
            fs[f, j] = part[16 * j : 16 * j + 16].astype(BF)
        to_owners(group, fs.at[f], fb.at[f], "f", HW, f)
        await_bytes(rb.at[f, 0:15], flag("es", f))

    for group in range(2):

        @pl.when(c == group)
        def _():
            for f in range(NC):
                combine(f, group)
            dense_columns(group)

    ready("norm_out")
    few = jnp.logical_and(c == 0, z < 4)

    @pl.when(few)
    def _():
        await_bytes(d4b.at[0:3], flag("d4r"))
        await_bytes(d4b.at[0:3], flag("d4s"))

    @pl.when(jnp.logical_not(few))
    def _():
        await_bytes(d4b, flag("d4r"))
        await_bytes(d4b, flag("d4s"))

    dense = jnp.concatenate([d4b[n] for n in range(4)], axis=1).astype(F32)
    dense = hb[:, own_half].astype(F32) + mixing * dense

    for f in range(NC):

        @pl.when(c == 0)
        def _():
            await_bytes(fb.at[f, 1:8], flag("f", "r", f))

        @pl.when(c == 1)
        def _():
            await_bytes(fb.at[f], flag("f", "r", f))

        piece = pl.ds(pl.multiple_of(c * 1024 + HW * f, HW), HW)
        fin[:, piece] = jnp.sum(fb[f].astype(F32), axis=0) + dense[:, HW * f : HW * f + HW]
        send(fin.at[:, piece], fin.at[:, piece], flag("us"), flag("ur"), mate)

    @pl.when(c == 0)
    def _():
        await_bytes(fb.at[:, 0:7], flag("f", "s"))

    @pl.when(c == 1)
    def _():
        await_bytes(fb, flag("f", "s"))

    await_bytes(fin.at[:, mate_half], flag("ur"))
    out[...] = norm(fin[...], norm_out[...]).astype(BF)
    await_bytes(fin.at[:, own_half], flag("us"))


def shards(
    tokens, cache_keys, cache_values, cache_lengths, norm_in, w_query, w_key, w_value,
    stick_bias, w_output, norm_mid, routes, route_weights, expert_gate, expert_up,
    expert_down, dense_gate, dense_up, dense_down, mix_gate, norm_out,
):
    vmem = pl.BlockSpec(memory_space=pltpu.VMEM)
    hbm = pl.BlockSpec(memory_space=pltpu.HBM)
    dma = pltpu.SemaphoreType.DMA
    V = pltpu.VMEM
    res = pl.pallas_call(
        body,
        out_shape=V((16, 2304), BF),
        in_specs=[hbm] * 21,
        out_specs=vmem,
        scratch_shapes=[
            V((16, 2048), BF),
            V((1, 2048), F32),
            V((2048, 256), BF),
            V((64, 2048), BF),
            V((64, 2048), BF),
            pltpu.SMEM((16,), jnp.int32),
            pltpu.SMEM((4,), F32),
            V((4, 256, 1024), BF),
            V((4, 256, 1024), BF),
            V((16, 256), BF),
            V((16, 256), BF),
            V((16, 256), BF),
            V((6, 16), jnp.int32),
            V((6, 16), F32),
            V((256, 2048), BF),
            V((1, 2048), F32),
            V((1, 2048), F32),
            V((2048, 256), BF),
            V((2048, 256), BF),
            V((256, 2048), BF),
            V((1, 2048), F32),
            V((2048, 256), BF),
            V((2048, 256), BF),
            V((256, 2048), BF),
            V((16, 2048), BF),
            V((16, 2048), F32),
            V((16, 2048), F32),
            V((NC, 4, 16, 2 * HW), BF),
            V((NC, 16, 8, 2 * HW), BF),
            V((NC, 16, 8, 2 * HW), BF),
            V((NC, 16, 8, 2 * HW), BF),
            V((NC, 16, 8, 2 * HW), BF),
            V((NC, 4, 16, 2 * HW), BF),
            V((NC, 8, 16, HW), BF),
            V((16, 2048), F32),
            V((16, 128), F32),
            V((8, 16, 128), F32),
            V((48, 256), BF),
            V((16, 48, 256), BF),
            V((4, 16, 512), BF),
            V((8, 16, 256), BF),
            V((16, 128), BF),
            V((4, 16, 256), BF),
            V((8, 16, 128), BF),
            V((4, 16, 256), BF),
            V((4, 16, 256), BF),
            V((128, 64), BF),
            V((64, 128), BF),
            V((64, 128), BF),
            V((4, 128, 256), F32),
            dma((27,)),
            dma((96,)),
        ],
        compiler_params=pltpu.CompilerParams(
            collective_id=0, has_side_effects=True, vmem_limit_bytes=56 * 1024 * 1024
        ),
    )(
        tokens,
        norm_in.reshape(1, -1),
        w_query,
        w_key.T,
        w_value.T,
        cache_lengths,
        stick_bias,
        cache_keys.reshape(4, 256, 1024),
        cache_values.reshape(4, 256, 1024),
        dense_gate,
        dense_up,
        dense_down.T,
        routes.T,
        route_weights.T,
        w_output,
        norm_mid.reshape(1, -1),
        mix_gate.reshape(1, -1),
        expert_gate.reshape(2048, 256),
        expert_up.reshape(2048, 256),
        expert_down.reshape(256, 2048),
        norm_out.reshape(1, -1),
    )
    return res[:, 0:2048], res[:, 2048:2112], res[:, 2176:2240]


def solution(mesh):
    split = Mesh(
        mesh.devices.reshape(NZ, NY, NX, mesh.shape["tp"]), ("ep_0", "ep_1", "ep_2", "tp")
    )
    return jax.shard_map(
        shards,
        mesh=split,
        in_specs=(
            P(EP, None),
            P(EP, "tp", None, None),
            P(EP, "tp", None, None),
            P(EP),
            P(),
            P(None, "tp"),
            P(None, "tp"),
            P(None, "tp"),
            P("tp"),
            P("tp", None),
            P(),
            P(EP, None),
            P(EP, None),
            P(EP, None, "tp"),
            P(EP, None, "tp"),
            P(EP, "tp", None),
            P(EP, None),
            P(EP, None),
            P(None, EP),
            P(),
            P(),
        ),
        out_specs=(P(EP, None), P(EP, "tp"), P(EP, "tp")),
        check_vma=False,
    )
```

```python
import jax
import jax.numpy as jnp
from jax import lax
from jax.experimental import pallas as pl
from jax.experimental.pallas import tpu as pltpu
from jax.sharding import Mesh
from jax.sharding import PartitionSpec as P

EP = ("ep_0", "ep_1", "ep_2")
MESH = pl.DeviceIdType.MESH
BF = jnp.bfloat16
F32 = jnp.float32
NZ, NY, NX = 8, 4, 4
PLANE = NY * NX
ORDER = (0, 1, 7, 2, 6, 3, 5, 4)
SLOT = {d: i for i, d in enumerate(ORDER)}
OFFS = sorted(
    ((dy, dx) for dy in range(NY) for dx in range(NX) if (dy, dx) != (0, 0)),
    key=lambda o: (-min(o[0], NY - o[0]) - min(o[1], NX - o[1]), (o[0] + o[1]) % 2, o[1]),
)
BACK = [OFFS.index(((-dy) % NY, (-dx) % NX)) for dy, dx in OFFS]
NP = len(OFFS)
NC = 4
HW = 1024 // NC


def dot(a, b):
    return jnp.dot(a, b, preferred_element_type=F32)


def dot_nt(a, b):
    return lax.dot_general(a, b, (((1,), (1,)), ((), ())), preferred_element_type=F32)


def rows(shape):
    return lax.broadcasted_iota(jnp.int32, shape, 0)


def cols(shape):
    return lax.broadcasted_iota(jnp.int32, shape, 1)


def ones_where(mask):
    return jnp.where(mask, 1.0, 0.0).astype(BF)


def norm(v, gain):
    center = jnp.mean(v, -1, keepdims=True)
    off = v - center
    spread = jnp.mean(off * off, -1, keepdims=True)
    return off * lax.rsqrt(spread + 1e-05) * gain


def halves(v):
    high = v.astype(BF)
    return high, (v - high.astype(F32)).astype(BF)


def body(
    tokens_h, norm_in_h, wq_h, wk_h, wv_h, lens_h, bias_h, ck, cv, dgate_h, dup_h, ddown_h,
    routes_h, weights_h, wo_h, norm_mid_h, mix_gate_h, eg_h, eu_h, ed_h, norm_out_h,
    res,
    tokens, norm_in, wq, wk, wv, lens, bias, kb, vb, dgate, dup, ddown,
    routes, weights, wo, norm_mid, mix_gate, eg, eu, ed, norm_out,
    egm, eum, edm, hb, pps, ppr, zb, ob, xb, eb, rb, fs, fb, fin,
    rts, rtb, dws, dwb, d2s, d2b, das, dab, d3m, d4s, d4b,
    pm, wh, wl, ga,
    lsem, bank,
):
    out, fk, fv = res.at[:, 0:2048], res.at[:, 2048:2112], res.at[:, 2176:2240]
    z, y, x, c = (lax.axis_index(a) for a in (*EP, "tp"))
    me = y * NX + x
    o = 1 - c
    mate = (z, y, x, o)

    def along(d):
        return (lax.rem(z + d, NZ), y, x, c)

    def across(k):
        dy, dx = OFFS[k]
        return (z, lax.rem(y + dy, NY), lax.rem(x + dx, NX), c)

    def place(k):
        dy, dx = OFFS[k]
        return lax.rem(y + dy, NY) * NX + lax.rem(x + dx, NX)

    flags = {}

    def flag(*name):
        return bank.at[flags.setdefault(name, len(flags))]

    def send(src, dst, out_flag, in_flag, dev):
        pltpu.make_async_remote_copy(
            src_ref=src, dst_ref=dst, send_sem=out_flag, recv_sem=in_flag,
            device_id=dev, device_id_type=MESH,
        ).start()

    def await_bytes(ref, name):
        pltpu.make_async_copy(ref, ref, name).wait()

    reads = {}

    def fetch(name, src, dst):
        copy = pltpu.make_async_copy(src, dst, lsem.at[len(reads)])
        copy.start()
        reads[name] = copy

    def ready(*names):
        for name in names:
            reads[name].wait()

    fetch("tokens", tokens_h, tokens)
    fetch("norm_in", norm_in_h, norm_in)
    fetch("wq", wq_h, wq)
    fetch("wk", wk_h, wk)
    fetch("wv", wv_h, wv)
    fetch("dgate", dgate_h, dgate)
    fetch("dup", dup_h, dup)
    fetch("ddown", ddown_h, ddown)
    fetch("routes", routes_h, routes)
    fetch("weights", weights_h, weights)
    for b in range(4):
        fetch(("k", b), ck.at[b], kb.at[b])
    fetch("lens", lens_h, lens)
    fetch("bias", bias_h, bias)
    for b in range(4):
        fetch(("v", b), cv.at[b], vb.at[b])
    fetch("wo", wo_h, wo)
    fetch("norm_mid", norm_mid_h, norm_mid)
    fetch("mix_gate", mix_gate_h, mix_gate)

    barrier = pltpu.get_barrier_semaphore()
    for d in range(1, NZ):
        pl.semaphore_signal(barrier, inc=1, device_id=along(d), device_id_type=MESH)
    for k in range(NP):
        pl.semaphore_signal(barrier, inc=1, device_id=across(k), device_id_type=MESH)
    pl.semaphore_signal(barrier, inc=1, device_id=mate, device_id_type=MESH)

    ready("tokens", "norm_in")
    normed = norm(tokens[...].astype(F32), norm_in[...]).astype(BF)
    ready("wq", "wk", "wv")
    queries = dot(normed, wq[...]).astype(BF)
    fk[...] = dot_nt(normed, wk[...]).astype(BF)
    fv[...] = dot_nt(normed, wv[...]).astype(BF)

    ready("dgate", "dup", "ddown", "routes", "weights")
    dws[0:16] = dgate[...]
    dws[16:32] = dup[...]
    dws[32:48] = ddown[...]
    rts[...] = jnp.zeros((16, 128), F32)
    for j in range(8):
        rts[0:6, 16 * j : 16 * j + 16] = routes[...].astype(F32)
        rts[8:14, 16 * j : 16 * j + 16] = weights[...]

    pl.semaphore_wait(barrier, NZ - 1 + NP + 1)
    for k in range(NP):
        send(dws, dwb.at[me], flag("ws"), flag("wr"), across(k))
    for d in ORDER[1:]:
        send(rts, rtb.at[SLOT[NZ - d]], flag("ts"), flag("tr"), along(d))
    dwb[me] = dws[...]
    rtb[0] = rts[...]

    wide = (64, 256)
    expand = ones_where(rows((64, 16)) // 4 == cols((64, 16)))
    fold = ones_where(lax.rem(rows((256, 256)), 64) == lax.rem(cols((256, 256)), 64))
    head_of = cols(wide) // 64 == lax.rem(rows(wide), 4)
    seq_of = cols(wide) // 64 == lax.rem(rows(wide) // 4, 4)
    picked = jnp.where(head_of, dot(expand, queries), 0.0).astype(BF)
    grid = jnp.where(seq_of, dot(picked, fold), 0.0).astype(BF)
    parts = []
    ready(*(("k", b) for b in range(4)))
    for b in range(4):
        parts.append(dot(grid[16 * b : 16 * b + 16], kb[b]))
    scores = jnp.concatenate(parts, axis=0) * 0.125
    ready("lens", "bias")
    row = rows((64, 128))
    length = jnp.zeros((64, 128), jnp.int32)
    for s in range(16):
        length = jnp.where(row // 4 == s, lens[s], length)
    offset = jnp.zeros((64, 128), F32)
    for g in range(4):
        offset = jnp.where(lax.rem(row, 4) == g, bias[g], offset)
    later = ones_where(rows((128, 128)) >= cols((128, 128)))
    zs, keeps, seen = [], [], []
    for n in range(8):
        zn = scores[:, 128 * n : 128 * n + 128] + offset
        vis = cols((64, 128)) + 128 * n < length
        soft = jnp.maximum(zn, 0.0) + jnp.log1p(jnp.exp(-jnp.abs(zn)))
        zs.append(zn)
        seen.append(vis)
        keeps.append(jnp.where(vis, soft, 0.0))
    high, low = halves(jnp.concatenate(keeps, axis=0))
    within = dot(high, later) + dot(low, later)
    carry = jnp.zeros((64, 1), F32)
    sticks = [None] * 8
    for n in range(7, -1, -1):
        w = within[64 * n : 64 * n + 64]
        sticks[n] = jnp.where(seen[n], jnp.exp(zs[n] - w - carry), 0.0).astype(BF)
        carry = carry + w[:, 0:1]
    stick = jnp.concatenate(sticks, axis=1)
    parts = []
    ready(*(("v", b) for b in range(4)))
    fetch("eg", eg_h, eg)
    fetch("eu", eu_h, eu)
    fetch("ed", ed_h, ed)
    fetch("norm_out", norm_out_h, norm_out)
    for b in range(4):
        parts.append(dot_nt(stick[16 * b : 16 * b + 16], vb[b]))
    att = jnp.where(seq_of, jnp.concatenate(parts, axis=0), 0.0).astype(BF)
    att = jnp.where(head_of, dot(att, fold), 0.0).astype(BF)
    gather = ones_where(cols((16, 64)) // 4 == rows((16, 64)))
    attended = dot(gather, att).astype(BF)
    ready("wo")
    pps[...] = dot(attended, wo[...])
    send(pps, ppr, flag("ps"), flag("pr"), mate)

    await_bytes(rtb.at[1:8], flag("tr"))
    shape = (128, 64)
    expert = (z * PLANE + rows(shape) // 8).astype(F32)
    ahead = ones_where(
        (rows((64, 64)) < cols((64, 64))) & (rows((64, 64)) // 16 == cols((64, 64)) // 16)
    )
    table = jnp.zeros((16, 64), F32)
    for j in range(4):
        table = jnp.where(cols((16, 64)) // 16 == j, rtb[4 * c + j][:, 0:64], table)
    hit = jnp.zeros(shape, F32)
    share = jnp.zeros(shape, F32)
    for k in range(6):
        same = table[k : k + 1] == expert
        hit = jnp.where(same, 1.0, hit)
        share = jnp.where(same, table[8 + k : 9 + k], share)
    rank = dot(hit.astype(BF), ahead)
    here = (
        (hit > 0.5)
        & (rank == lax.rem(rows(shape), 2).astype(F32))
        & (cols(shape) // 16 == lax.rem(rows(shape), 8) // 2)
    )
    pm[...] = ones_where(here)
    wh[...], wl[...] = halves(jnp.transpose(jnp.where(here, share, 0.0)))
    await_bytes(rtb.at[1:8], flag("ts"))
    await_bytes(dwb.at[0:15], flag("ws"))

    own_half = pl.ds(pl.multiple_of(c * 1024, 1024), 1024)
    mate_half = pl.ds(pl.multiple_of(o * 1024, 1024), 1024)
    ready("norm_mid", "mix_gate")
    await_bytes(ppr, flag("pr"))
    hidden = norm(normed.astype(F32) + (pps[...] + ppr[...]), norm_mid[...]).astype(BF)
    hb[...] = hidden
    lanes = pl.ds(pl.multiple_of(c * HW, HW), HW)
    for f, d in [(f, d) for f in range(NC) for d in (4, 5, 3, 6, 2, 7, 1)]:
        source = hb.at[:, pl.ds(pl.multiple_of(c * 1024 + f * HW, HW), HW)]
        t = SLOT[NZ - d]
        there = (lax.rem(z + d, NZ), y, x, t // 4)
        send(source, zb.at[f, t % 4, :, lanes], flag("zs"), flag("zr", f), there)

    @pl.when(c == 0)
    def _():
        for f in range(NC):
            for h in range(2):
                at = 1024 * h + HW * f
                zb[f, 0, :, HW * h : HW * h + HW] = hb[:, at : at + HW]

    mixing = jax.nn.sigmoid(jnp.sum(hidden.astype(F32) * mix_gate[...], -1, keepdims=True))
    await_bytes(pps, flag("ps"))
    ready("eg", "eu", "ed")
    send(eg, egm, flag("g0s"), flag("g0r"), mate)
    send(eu, eum, flag("g1s"), flag("g1r"), mate)
    send(ed, edm, flag("g2s"), flag("g2r"), mate)

    for f in range(NC):

        @pl.when(c == 0)
        def _():
            await_bytes(zb.at[f, 1:4], flag("zr", f))

        @pl.when(c == 1)
        def _():
            await_bytes(zb.at[f], flag("zr", f))

        going = dot(pm[...], zb[f].reshape(64, 2 * HW))
        for q in range(PLANE):
            ob[f, q] = going[8 * q : 8 * q + 8].astype(BF)
        for k in range(NP):
            send(ob.at[f, place(k)], xb.at[f, me], flag("xs", f), flag("xr", f), across(k))
        xb[f, me] = ob[f, me]

    inner = lax.rem(z, 4) * 256
    features = pl.ds(pl.multiple_of((z // 4) * HW + lax.rem(inner, HW), 256), 256)
    column = zb[inner // HW, :, :, features].reshape(64, 256)
    await_bytes(dwb.at[0:15], flag("wr"))
    pre = dot(column, dwb[:, 0:16, :].reshape(256, 256))
    lin = dot(column, dwb[:, 16:32, :].reshape(256, 256))
    for j in range(4):
        for h in range(2):
            for i, v in enumerate((pre, lin)):
                at = 256 * h + 128 * i
                d2s[j, :, at : at + 128] = v[16 * j : 16 * j + 16, 128 * h : 128 * h + 128].astype(BF)

    def to_owners(group, source, target, name, width, f):
        for j in (3, 2, 1, 0):
            d = ORDER[4 * group + j]
            for h in range(2):
                piece = source.at[j, :, width * h : width * h + width]
                slot = target.at[SLOT[(NZ - d) % NZ]]
                if d:
                    there = (lax.rem(z + d, NZ), y, x, h)
                elif h:
                    there = mate
                else:
                    target[0] = source[j, :, 0:width]
                    continue
                send(piece, slot, flag(name, "s"), flag(name, "r", f), there)

    pl.when(c == 0)(lambda: to_owners(0, d2s, d2b, "d2", 256, 0))
    pl.when(c == 1)(lambda: to_owners(1, d2s, d2b, "d2", 256, 0))
    await_bytes(fb.at[:, 1:8], flag("zs"))
    await_bytes(egm, flag("g0s"))
    await_bytes(eum, flag("g1s"))
    await_bytes(edm, flag("g2s"))
    await_bytes(egm, flag("g0r"))
    await_bytes(eum, flag("g1r"))
    await_bytes(edm, flag("g2r"))

    sums = [None] * 4
    for f in range(NC):
        await_bytes(xb.at[f, 0:15], flag("xr", f))
        arrived = xb[f].reshape(128, 2 * HW)
        for i, ref in enumerate((eg, eu, egm, eum)):
            step = dot(arrived[:, 0:HW], ref[HW * f : HW * f + HW])
            step = step + dot(arrived[:, HW : 2 * HW], ref[1024 + HW * f : 1024 + HW * f + HW])
            if f > 0:
                step = step + ga[i]
            if f < NC - 1:
                ga[i] = step
            sums[i] = step
    acts = [(jax.nn.silu(sums[i]) * sums[i + 1]).astype(BF) for i in (0, 2)]
    for f in range(NC):
        for h in range(2):
            at = 1024 * h + HW * f
            total = dot(acts[0], ed[:, at : at + HW]).astype(BF).astype(F32)
            total = total + dot(acts[1], edm[:, at : at + HW]).astype(BF).astype(F32)
            for q in range(PLANE):
                eb[f, q, :, HW * h : HW * h + HW] = total[8 * q : 8 * q + 8].astype(BF)
        for k in range(NP):
            send(eb.at[f, place(k)], rb.at[f, me], flag("es", f), flag("er", f), across(k))
        rb[f, me] = eb[f, me]
    for f in range(NC):
        await_bytes(xb.at[f, 0:15], flag("xs", f))

    @pl.when(c == 0)
    def _():
        await_bytes(d2b.at[1:8], flag("d2", "r", 0))
        await_bytes(d2b.at[1:8], flag("d2", "s"))

    @pl.when(c == 1)
    def _():
        await_bytes(d2b, flag("d2", "r", 0))
        await_bytes(d2b, flag("d2", "s"))

    summed = jnp.sum(d2b[...].astype(F32), axis=0)
    das[...] = (jax.nn.silu(summed[:, 0:128]) * summed[:, 128:256]).astype(BF)
    lanes = pl.ds(pl.multiple_of(c * 128, 128), 128)
    for d in ORDER[1:]:
        t = SLOT[NZ - d]
        there = (lax.rem(z + d, NZ), y, x, t // 4)
        send(das, dab.at[t % 4, :, lanes], flag("d3s"), flag("d3r"), there)

    @pl.when(c == 0)
    def _():
        dab[0, :, 0:128] = das[...]

    @pl.when(c == 1)
    def _():
        send(das, dab.at[0, :, 128:256], flag("d3s"), flag("d3r"), mate)

    def dense_columns(group):
        if group == 0:
            await_bytes(d3m.at[0:7], flag("d3r"))
            await_bytes(d3m.at[0:7], flag("d3s"))
        else:
            await_bytes(d3m, flag("d3r"))
            await_bytes(d3m, flag("d3s"))
        block = dot_nt(dab[...].reshape(64, 256), dwb[:, 32:48, :].reshape(256, 256))
        spot = lax.rem(z, 4)
        for j in range(4):
            d = ORDER[4 * group + j]
            d4s[j] = block[16 * j : 16 * j + 16].astype(BF)
            if d:
                there = (lax.rem(z + d, NZ), y, x, z // 4)
                send(d4s.at[j], d4b.at[spot], flag("d4s"), flag("d4r"), there)
                continue

            @pl.when(z < 4)
            def _():
                d4b[spot] = d4s[j]

            @pl.when(z >= 4)
            def _():
                send(d4s.at[j], d4b.at[spot], flag("d4s"), flag("d4r"), mate)

    def combine(f, group):
        await_bytes(rb.at[f, 0:15], flag("er", f))
        block = rb[f].reshape(128, 2 * HW)
        part = dot(wh[...], block) + dot(wl[...], block)
        for j in range(4):
            fs[f, j] = part[16 * j : 16 * j + 16].astype(BF)
        to_owners(group, fs.at[f], fb.at[f], "f", HW, f)
        await_bytes(rb.at[f, 0:15], flag("es", f))

    for group in range(2):

        @pl.when(c == group)
        def _():
            for f in range(NC):
                combine(f, group)
            dense_columns(group)

    ready("norm_out")
    few = jnp.logical_and(c == 0, z < 4)

    @pl.when(few)
    def _():
        await_bytes(d4b.at[0:3], flag("d4r"))
        await_bytes(d4b.at[0:3], flag("d4s"))

    @pl.when(jnp.logical_not(few))
    def _():
        await_bytes(d4b, flag("d4r"))
        await_bytes(d4b, flag("d4s"))

    dense = jnp.concatenate([d4b[n] for n in range(4)], axis=1).astype(F32)
    dense = hb[:, own_half].astype(F32) + mixing * dense

    for f in range(NC):

        @pl.when(c == 0)
        def _():
            await_bytes(fb.at[f, 1:8], flag("f", "r", f))

        @pl.when(c == 1)
        def _():
            await_bytes(fb.at[f], flag("f", "r", f))

        piece = pl.ds(pl.multiple_of(c * 1024 + HW * f, HW), HW)
        fin[:, piece] = jnp.sum(fb[f].astype(F32), axis=0) + dense[:, HW * f : HW * f + HW]
        send(fin.at[:, piece], fin.at[:, piece], flag("us"), flag("ur"), mate)

    @pl.when(c == 0)
    def _():
        await_bytes(fb.at[:, 0:7], flag("f", "s"))

    @pl.when(c == 1)
    def _():
        await_bytes(fb, flag("f", "s"))

    await_bytes(fin.at[:, mate_half], flag("ur"))
    out[...] = norm(fin[...], norm_out[...]).astype(BF)
    await_bytes(fin.at[:, own_half], flag("us"))


def shards(
    tokens, cache_keys, cache_values, cache_lengths, norm_in, w_query, w_key, w_value,
    stick_bias, w_output, norm_mid, routes, route_weights, expert_gate, expert_up,
    expert_down, dense_gate, dense_up, dense_down, mix_gate, norm_out,
):
    vmem = pl.BlockSpec(memory_space=pltpu.VMEM)
    hbm = pl.BlockSpec(memory_space=pltpu.HBM)
    dma = pltpu.SemaphoreType.DMA
    V = pltpu.VMEM
    res = pl.pallas_call(
        body,
        out_shape=V((16, 2304), BF),
        in_specs=[hbm] * 21,
        out_specs=vmem,
        scratch_shapes=[
            V((16, 2048), BF),
            V((1, 2048), F32),
            V((2048, 256), BF),
            V((64, 2048), BF),
            V((64, 2048), BF),
            pltpu.SMEM((16,), jnp.int32),
            pltpu.SMEM((4,), F32),
            V((4, 256, 1024), BF),
            V((4, 256, 1024), BF),
            V((16, 256), BF),
            V((16, 256), BF),
            V((16, 256), BF),
            V((6, 16), jnp.int32),
            V((6, 16), F32),
            V((256, 2048), BF),
            V((1, 2048), F32),
            V((1, 2048), F32),
            V((2048, 256), BF),
            V((2048, 256), BF),
            V((256, 2048), BF),
            V((1, 2048), F32),
            V((2048, 256), BF),
            V((2048, 256), BF),
            V((256, 2048), BF),
            V((16, 2048), BF),
            V((16, 2048), F32),
            V((16, 2048), F32),
            V((NC, 4, 16, 2 * HW), BF),
            V((NC, 16, 8, 2 * HW), BF),
            V((NC, 16, 8, 2 * HW), BF),
            V((NC, 16, 8, 2 * HW), BF),
            V((NC, 16, 8, 2 * HW), BF),
            V((NC, 4, 16, 2 * HW), BF),
            V((NC, 8, 16, HW), BF),
            V((16, 2048), F32),
            V((16, 128), F32),
            V((8, 16, 128), F32),
            V((48, 256), BF),
            V((16, 48, 256), BF),
            V((4, 16, 512), BF),
            V((8, 16, 256), BF),
            V((16, 128), BF),
            V((4, 16, 256), BF),
            V((8, 16, 128), BF),
            V((4, 16, 256), BF),
            V((4, 16, 256), BF),
            V((128, 64), BF),
            V((64, 128), BF),
            V((64, 128), BF),
            V((4, 128, 256), F32),
            dma((27,)),
            dma((96,)),
        ],
        compiler_params=pltpu.CompilerParams(
            collective_id=0, has_side_effects=True, vmem_limit_bytes=56 * 1024 * 1024
        ),
    )(
        tokens,
        norm_in.reshape(1, -1),
        w_query,
        w_key.T,
        w_value.T,
        cache_lengths,
        stick_bias,
        cache_keys.reshape(4, 256, 1024),
        cache_values.reshape(4, 256, 1024),
        dense_gate,
        dense_up,
        dense_down.T,
        routes.T,
        route_weights.T,
        w_output,
        norm_mid.reshape(1, -1),
        mix_gate.reshape(1, -1),
        expert_gate.reshape(2048, 256),
        expert_up.reshape(2048, 256),
        expert_down.reshape(256, 2048),
        norm_out.reshape(1, -1),
    )
    return res[:, 0:2048], res[:, 2048:2112], res[:, 2176:2240]


def solution(mesh):
    split = Mesh(
        mesh.devices.reshape(NZ, NY, NX, mesh.shape["tp"]), ("ep_0", "ep_1", "ep_2", "tp")
    )
    return jax.shard_map(
        shards,
        mesh=split,
        in_specs=(
            P(EP, None),
            P(EP, "tp", None, None),
            P(EP, "tp", None, None),
            P(EP),
            P(),
            P(None, "tp"),
            P(None, "tp"),
            P(None, "tp"),
            P("tp"),
            P("tp", None),
            P(),
            P(EP, None),
            P(EP, None),
            P(EP, None, "tp"),
            P(EP, None, "tp"),
            P(EP, "tp", None),
            P(EP, None),
            P(EP, None),
            P(None, EP),
            P(),
            P(),
        ),
        out_specs=(P(EP, None), P(EP, "tp"), P(EP, "tp")),
        check_vma=False,
    )
```
